32 devices in a mesh: ep: 8 (over z, core), tp: 4 (over y, x).
Axes of the slice: x: 2, y: 2, z: 4, core: 2. Of those that a mesh axis runs over, the one named last changes fastest.
Arguments:
- stream: bfloat16 [128, 4096], P('ep'), may hold values from -6 to 6
- previous_state: float32 [128, 128, 4096], P('ep', None, 'tp'), may hold values from -6 to 6
- mixer_norm_gain: float32 [4096], replicated, may hold values from 0.1 to 1.9
- query_matrix: bfloat16 [4096, 2048], P('ep'), may hold values from -0.09375 to 0.09375
- key_matrix: bfloat16 [4096, 2048], P('ep'), may hold values from -0.09375 to 0.09375
- value_matrix: bfloat16 [4096, 4096], P('ep', 'tp'), may hold values from -0.09375 to 0.09375
- output_gate_weight: bfloat16 [4096, 4096], P('ep', 'tp'), may hold values from -0.09375 to 0.09375
- decay_lower_factor: bfloat16 [4096, 64], replicated, may hold values from -0.09375 to 0.09375
- decay_upper_factor: bfloat16 [64, 2048], replicated, may hold values from -3 to 3
- forgetting_boost: float32 [128, 2048], P('ep'), may hold values from 0.02 to 1.5
- head_norm_gain: float32 [256], replicated, may hold values from 0.1 to 1.9
- output_matrix: bfloat16 [4096, 4096], P('tp'), may hold values from -0.1875 to 0.1875
- mixture_norm_gain: float32 [4096], replicated, may hold values from 0.1 to 1.9
- expert_gate_weight: bfloat16 [8, 1024, 4096], P('ep', 'tp'), may hold values from -0.09375 to 0.09375
- expert_up_weight: bfloat16 [8, 1024, 4096], P('ep', 'tp'), may hold values from -0.09375 to 0.09375
- expert_down_weight: bfloat16 [8, 1024, 4096], P('ep', None, 'tp'), may hold values from -0.375 to 0.375
- expert_index_table: int32 [128, 2], P('ep'), may hold values from 0 to 7, as said below
- expert_scores_within: float32 [128, 2], P('ep'), may hold values from -6 to 6
- group_probability: float32 [128], P('ep'), may hold values from 0.3 to 1
Outputs:
- new_stream: bfloat16 [128, 4096], P('ep', 'tp')
- new_state: float32 [128, 128, 4096], P('ep', None, 'tp')
The draws below stay inside these ranges and needn't reach their ends.
Inputs may be any that keep to these rules, and one draw needn't show every extreme that they name: `expert_index_table`: the 2 experts of a sequence are distinct and lie in one group of 2 consecutive experts. Among the 16 sequences of one index of ep (aligned blocks of rows), each expert is named at most 8 times, and in every block some experts are named exactly 8 times.
All inputs are finite; a program needn't handle non-finite values.
Results may differ from the reference program's by a relative error of at most 0.02.
Values may be sent and summed in bfloat16 or wider, within the bound.
A program may use at most 128 MiB of HBM per device.

```python
import math
import jax
import jax.numpy as jnp
from jax import lax

D = 4096
HEAD_TOTAL = 16
KEY_CHANNELS = 128
DV = 256
RANK = 64
FF = 1024
GROUPS = 4
TOPK = 2
SEQ_DEV = 16
SEQUENCE_TOTAL = 128
EXPERTS = 8
PER_GROUP = 2
CAP = 8
N_EP = 8


def shuffle(subkey):
    return jax.random.permutation(subkey, SEQ_DEV)


def draw_expert_index_table(key, part):
    blocks = SEQUENCE_TOTAL // SEQ_DEV
    hot_count = PER_GROUP * CAP // TOPK
    key_hot, key_other, key_perm, key_turn = jax.random.split(jax.random.fold_in(key, 11), 4)
    hot_group = jax.random.randint(key_hot, (), 0, GROUPS)
    offsets = jax.random.randint(key_other, (blocks, SEQ_DEV), 1, GROUPS)
    orders = jax.vmap(shuffle)(jax.random.split(key_perm, blocks))
    places = jnp.arange(SEQ_DEV)
    chosen = (orders[:, :, None] == places[None, None, :]) & (places[None, :, None] < hot_count)
    is_hot = jnp.any(chosen, axis=1)
    group_id = jnp.where(is_hot, hot_group, (hot_group + offsets) % GROUPS)
    same_group = group_id[:, :, None] == group_id[:, None, :]
    before = places[None, :] < places[:, None]
    rank_in = jnp.sum(same_group & before[None], axis=2)
    rotation = jax.random.randint(key_turn, (blocks, GROUPS), 0, PER_GROUP)
    member = group_id[:, :, None] == jnp.arange(GROUPS)[None, None, :]
    shift_by = jnp.sum(jnp.where(member, rotation[:, None, :], 0), axis=2)
    within = (shift_by[:, :, None] + rank_in[:, :, None] * TOPK + jnp.arange(TOPK)[None, None, :]) % PER_GROUP
    chosen_ids = group_id[:, :, None] * PER_GROUP + within
    return chosen_ids.reshape(SEQUENCE_TOTAL, TOPK).astype(jnp.int32)


def block_scale(rng, dims, pieces, least, high):
    def one(position, shards_of):
        steps = jax.random.uniform(jax.random.fold_in(jax.random.fold_in(rng, 6), position), (shards_of,), jnp.float32, least / len(pieces), high / len(pieces))
        return jnp.repeat(jnp.exp(steps), dims[position] // shards_of).reshape((-1,) + (1,) * (len(dims) - position - 1))

    level = one(*pieces[0])
    for cut in pieces[1:]:
        level = level * one(*cut)
    return level


def centred(stream_key, dims, width, limit, cuts=(), kind=jnp.bfloat16):
    result = jax.random.normal(stream_key, dims, jnp.float32) * width
    if len(cuts) > 0:
        result = block_scale(stream_key, dims, cuts, -0.22, 0.18) * result
    return jnp.clip(result, min=-limit, max=limit).astype(kind)


def setup_inputs(seed: int = 0) -> dict:
    key_list = jax.random.split(jax.random.key(seed), 20)
    return {
        "stream": centred(key_list[0], (SEQUENCE_TOTAL, D), 1.0, 6.0, ((0, 8),)),
        "previous_state": centred(key_list[1], (SEQUENCE_TOTAL, KEY_CHANNELS, HEAD_TOTAL * DV), 1.0, 6.0, ((0, 8), (2, 4)), jnp.float32),
        "mixer_norm_gain": jnp.clip(1.0 + 0.18 * jax.random.normal(key_list[2], (D,), jnp.float32), 0.1, 1.9),
        "query_matrix": centred(key_list[3], (D, HEAD_TOTAL * KEY_CHANNELS), D ** -0.5, 0.09375, ((0, 8),)),
        "key_matrix": centred(key_list[4], (D, HEAD_TOTAL * KEY_CHANNELS), D ** -0.5, 0.09375, ((0, 8),)),
        "value_matrix": centred(key_list[5], (D, HEAD_TOTAL * DV), D ** -0.5, 0.09375, ((0, 8), (1, 4))),
        "output_gate_weight": centred(key_list[6], (D, HEAD_TOTAL * DV), D ** -0.5, 0.09375, ((0, 8), (1, 4))),
        "decay_lower_factor": centred(key_list[7], (D, RANK), D ** -0.5, 0.09375),
        "decay_upper_factor": centred(key_list[8], (RANK, HEAD_TOTAL * KEY_CHANNELS), (RANK // 16) ** -0.5, 3.0),
        "forgetting_boost": jnp.clip(jnp.exp(math.log(1.5) - 4.317488 * jax.random.uniform(key_list[9], (SEQUENCE_TOTAL, HEAD_TOTAL * KEY_CHANNELS), jnp.float32) ** block_scale(key_list[9], (SEQUENCE_TOTAL, HEAD_TOTAL * KEY_CHANNELS), ((0, 8),), -0.2, 0.2)), 0.02, 1.5),
        "head_norm_gain": jnp.clip(1.0 + 0.18 * jax.random.normal(key_list[10], (DV,), jnp.float32), 0.1, 1.9),
        "output_matrix": centred(key_list[11], (HEAD_TOTAL * DV, D), (HEAD_TOTAL * DV // 4) ** -0.5, 0.1875, ((0, 4),)),
        "mixture_norm_gain": jnp.clip(1.0 + 0.18 * jax.random.normal(key_list[12], (D,), jnp.float32), 0.1, 1.9),
        "expert_gate_weight": centred(key_list[13], (EXPERTS, FF, D), D ** -0.5, 0.09375, ((0, 8), (1, 4))),
        "expert_up_weight": centred(key_list[14], (EXPERTS, FF, D), D ** -0.5, 0.09375, ((0, 8), (1, 4))),
        "expert_down_weight": centred(key_list[15], (EXPERTS, FF, D), (FF // 4) ** -0.5, 0.375, ((0, 8), (2, 4))),
        "expert_index_table": draw_expert_index_table(jax.random.fold_in(key_list[19], 71), 0),
        "expert_scores_within": centred(key_list[17], (SEQUENCE_TOTAL, TOPK), 1.5, 6.0, ((0, 8),), jnp.float32),
        "group_probability": jnp.clip(0.3 + 0.7 * jax.random.uniform(key_list[18], (SEQUENCE_TOTAL,), jnp.float32) ** block_scale(key_list[18], (SEQUENCE_TOTAL,), ((0, 8),), -0.2, 0.2), 0.3, 1.0),
    }


epsilon = 1e-06
forgetting_softness = 16.0

def rms_scaled(values, gain_vec):
    floats = values.astype(jnp.float32)
    scaled = floats * lax.rsqrt(lax.optimization_barrier(jnp.mean(floats * floats, axis=-1, keepdims=True)) + epsilon)
    return (scaled * gain_vec).astype(jnp.bfloat16)

def expert_apply(inputs):
    tokens_in, gate_mat, up_mat, down_mat = inputs
    gate_pre = jnp.dot(tokens_in, gate_mat.T, preferred_element_type=jnp.float32)
    up_pre = jnp.dot(tokens_in, up_mat.T, preferred_element_type=jnp.float32)
    hidden = (jax.nn.silu(gate_pre) * up_pre).astype(jnp.bfloat16)
    return jnp.dot(hidden, down_mat, preferred_element_type=jnp.float32).astype(jnp.bfloat16)

def reference(stream, previous_state, mixer_norm_gain, query_matrix, key_matrix, value_matrix, output_gate_weight, decay_lower_factor, decay_upper_factor, forgetting_boost, head_norm_gain, output_matrix, mixture_norm_gain, expert_gate_weight, expert_up_weight, expert_down_weight, expert_index_table, expert_scores_within, group_probability):
    normed = rms_scaled(stream, mixer_norm_gain)
    queries = (jnp.dot(normed, query_matrix, preferred_element_type=jnp.float32) * KEY_CHANNELS ** (-0.5)).astype(jnp.bfloat16)
    key_rows = jnp.dot(normed, key_matrix, preferred_element_type=jnp.float32).astype(jnp.bfloat16)
    value_rows = jnp.dot(normed, value_matrix, preferred_element_type=jnp.float32).astype(jnp.bfloat16)
    gate_rows = jnp.dot(normed, output_gate_weight, preferred_element_type=jnp.float32).astype(jnp.bfloat16)
    low_rank = jnp.dot(normed, decay_lower_factor, preferred_element_type=jnp.float32).astype(jnp.bfloat16)
    forgetting_logit = jnp.dot(low_rank, decay_upper_factor, preferred_element_type=jnp.float32)
    forgetting_lograte = jax.nn.log_sigmoid(forgetting_logit) / forgetting_softness - forgetting_boost
    factor = jnp.exp(forgetting_lograte).reshape(SEQUENCE_TOTAL, HEAD_TOTAL, KEY_CHANNELS).transpose(0, 2, 1)[..., None]
    state_four = previous_state.reshape(SEQUENCE_TOTAL, KEY_CHANNELS, HEAD_TOTAL, DV)
    key_part = key_rows.astype(jnp.float32).reshape(SEQUENCE_TOTAL, HEAD_TOTAL, KEY_CHANNELS).transpose(0, 2, 1)[..., None]
    value_part = value_rows.astype(jnp.float32).reshape(SEQUENCE_TOTAL, 1, HEAD_TOTAL, DV)
    updated = factor * state_four + key_part * value_part
    query_part = queries.astype(jnp.float32).reshape(SEQUENCE_TOTAL, HEAD_TOTAL, KEY_CHANNELS).transpose(0, 2, 1)
    readout = jnp.einsum('skh,skhv->shv', query_part, updated, precision=lax.Precision.HIGHEST)
    mean_sq = lax.optimization_barrier(jnp.mean(readout * readout, axis=-1, keepdims=True))
    gate_part = jax.nn.silu(gate_rows.astype(jnp.float32).reshape(SEQUENCE_TOTAL, HEAD_TOTAL, DV))
    gated_rows = (readout * lax.rsqrt(mean_sq + epsilon) * head_norm_gain * gate_part).reshape(SEQUENCE_TOTAL, HEAD_TOTAL * DV).astype(jnp.bfloat16)
    blended_tokens = (stream.astype(jnp.float32) + jnp.dot(gated_rows, output_matrix, preferred_element_type=jnp.float32)).astype(jnp.bfloat16)
    normed_two = rms_scaled(blended_tokens, mixture_norm_gain)
    logit_exp = jnp.exp(expert_scores_within)
    weights = logit_exp / lax.optimization_barrier(jnp.sum(logit_exp, axis=-1, keepdims=True)) * group_probability[:, None]
    blocked = expert_index_table.reshape(N_EP, SEQ_DEV * TOPK).astype(jnp.int32)
    one_hot = (blocked[..., None] == jnp.arange(EXPERTS, dtype=jnp.int32)).astype(jnp.int32)
    rank_in = lax.optimization_barrier(jnp.sum(one_hot * (jnp.cumsum(one_hot, axis=1) - 1), axis=-1))
    column = (jnp.arange(N_EP, dtype=jnp.int32)[:, None] * CAP + rank_in).astype(jnp.int32)
    repeated = jnp.broadcast_to(normed_two.reshape(N_EP, SEQ_DEV, 1, D), (N_EP, SEQ_DEV, TOPK, D)).reshape(N_EP, SEQ_DEV * TOPK, D)
    buffer = jnp.zeros((EXPERTS, N_EP * CAP, D), jnp.bfloat16).at[blocked, column].set(repeated)
    results = lax.map(expert_apply, (buffer, expert_gate_weight, expert_up_weight, expert_down_weight))
    picked = results[blocked, column].reshape(SEQUENCE_TOTAL, TOPK, D)
    mixture = lax.optimization_barrier(jnp.sum(weights[..., None] * picked.astype(jnp.float32), axis=1))
    new_stream = (blended_tokens.astype(jnp.float32) + mixture).astype(jnp.bfloat16)
    return (new_stream, updated.reshape(SEQUENCE_TOTAL, KEY_CHANNELS, HEAD_TOTAL * DV))
```

```python
import functools

import jax
import jax.numpy as jnp
from jax import lax
from jax.experimental import pallas as pl
from jax.experimental.pallas import tpu as pltpu
from jax.sharding import PartitionSpec as P

HEAD_TOTAL = 16
KEY_CHANNELS = 128
DV = 256
GROUPS = 4
STEP = 2
F32 = jnp.float32
BF16 = jnp.bfloat16
MESH = pl.DeviceIdType.MESH

epsilon = 1e-06
forgetting_softness = 16.0


def rms_scaled(values, gain_vec):
    floats = values.astype(jnp.float32)
    scaled = floats * lax.rsqrt(jnp.mean(floats * floats, axis=-1, keepdims=True) + epsilon)
    return (scaled * gain_vec).astype(jnp.bfloat16)


def general(
    stream,
    previous_state,
    mixer_norm_gain,
    query_matrix,
    key_matrix,
    value_matrix,
    output_gate_weight,
    decay_lower_factor,
    decay_upper_factor,
    forgetting_boost,
    head_norm_gain,
    output_matrix,
    mixture_norm_gain,
    expert_gate_weight,
    expert_up_weight,
    expert_down_weight,
    expert_index_table,
    expert_scores_within,
    group_probability,
):
    seq_count, model_width = stream.shape
    value_local = previous_state.shape[2]
    head_count = max(1, value_local // DV)
    head_width = min(value_local, DV)
    tp_index = lax.axis_index("tp")
    leading_head = tp_index * value_local // DV
    value_start = tp_index * value_local % DV
    key_column_span = head_count * KEY_CHANNELS
    normed = rms_scaled(stream, mixer_norm_gain)
    own_query = lax.dynamic_slice_in_dim(
        query_matrix, leading_head * KEY_CHANNELS, key_column_span, 1
    )
    own_key = lax.dynamic_slice_in_dim(key_matrix, leading_head * KEY_CHANNELS, key_column_span, 1)
    spread = lax.all_to_all(normed, "ep", split_axis=1, concat_axis=0, tiled=True)
    joined = jnp.concatenate([own_query, own_key, value_matrix, output_gate_weight], axis=1)
    summed = lax.psum_scatter(
        jnp.dot(spread, joined, preferred_element_type=jnp.float32),
        "ep",
        scatter_dimension=0,
        tiled=True,
    )
    query_sum = summed[:, :key_column_span]
    key_sum = summed[:, key_column_span : 2 * key_column_span]
    value_sum = summed[:, 2 * key_column_span : 2 * key_column_span + value_local]
    gate_sum = summed[:, 2 * key_column_span + value_local :]
    queries = (query_sum * KEY_CHANNELS ** (-0.5)).astype(jnp.bfloat16)
    key_rows = key_sum.astype(jnp.bfloat16)
    value_rows = value_sum.astype(jnp.bfloat16)
    gate_rows = gate_sum.astype(jnp.bfloat16)
    low_rank = jnp.dot(normed, decay_lower_factor, preferred_element_type=jnp.float32).astype(
        jnp.bfloat16
    )
    local_expand_matrix = lax.dynamic_slice_in_dim(
        decay_upper_factor, leading_head * KEY_CHANNELS, key_column_span, 1
    )
    forgetting_logit = jnp.dot(low_rank, local_expand_matrix, preferred_element_type=jnp.float32)
    request_boost = lax.dynamic_slice_in_dim(
        forgetting_boost, leading_head * KEY_CHANNELS, key_column_span, 1
    )
    forgetting_lograte = jax.nn.log_sigmoid(forgetting_logit) / forgetting_softness - request_boost
    factor = (
        jnp.exp(forgetting_lograte)
        .reshape(seq_count, head_count, KEY_CHANNELS)
        .transpose(0, 2, 1)[..., None]
    )
    state_four = previous_state.reshape(seq_count, KEY_CHANNELS, head_count, head_width)
    key_part = (
        key_rows.astype(jnp.float32)
        .reshape(seq_count, head_count, KEY_CHANNELS)
        .transpose(0, 2, 1)[..., None]
    )
    value_part = value_rows.astype(jnp.float32).reshape(seq_count, 1, head_count, head_width)
    updated = factor * state_four + key_part * value_part
    query_part = (
        queries.astype(jnp.float32).reshape(seq_count, head_count, KEY_CHANNELS).transpose(0, 2, 1)
    )
    readout = jnp.einsum("skh,skhv->shv", query_part, updated, precision=lax.Precision.HIGHEST)
    square_sums = jnp.sum(readout * readout, axis=-1)
    norm_table = lax.dynamic_update_slice(
        jnp.zeros((seq_count, HEAD_TOTAL), jnp.float32), square_sums, (jnp.int32(0), leading_head)
    )
    totals = lax.psum(norm_table, "tp")
    own_totals = lax.dynamic_slice_in_dim(totals, leading_head, head_count, 1)
    mean_sq = own_totals[..., None] / DV
    own_gain = lax.dynamic_slice_in_dim(head_norm_gain, value_start, head_width, 0)
    gate_part = jax.nn.silu(
        gate_rows.astype(jnp.float32).reshape(seq_count, head_count, head_width)
    )
    gated_rows = (
        (readout * lax.rsqrt(mean_sq + epsilon) * own_gain * gate_part)
        .reshape(seq_count, value_local)
        .astype(jnp.bfloat16)
    )
    partial_out = jnp.dot(gated_rows, output_matrix, preferred_element_type=jnp.float32)
    mixer_sum = lax.psum(partial_out.astype(jnp.bfloat16), "tp").astype(jnp.float32)
    blended_tokens = (stream.astype(jnp.float32) + mixer_sum).astype(jnp.bfloat16)
    normed_two = rms_scaled(blended_tokens, mixture_norm_gain)
    ep_count = lax.axis_size("ep")
    local_experts = expert_gate_weight.shape[0]
    experts_all = ep_count * local_experts
    route_count = expert_index_table.shape[1]
    capacity = 2 * seq_count * route_count // experts_all
    slot_count = experts_all * capacity
    flat_ids = expert_index_table.reshape(seq_count * route_count)
    one_hot = (flat_ids[:, None] == jnp.arange(experts_all, dtype=jnp.int32)[None, :]).astype(
        jnp.int32
    )
    rank_in = jnp.sum(one_hot * (jnp.cumsum(one_hot, axis=0) - 1), axis=1)
    place_lookup = flat_ids * capacity + rank_in
    placing = (place_lookup[:, None] == jnp.arange(slot_count, dtype=jnp.int32)[None, :]).astype(
        jnp.float32
    )
    placing = placing.reshape(seq_count, route_count, slot_count)
    logit_exp = jnp.exp(expert_scores_within)
    weights = logit_exp / jnp.sum(logit_exp, axis=-1, keepdims=True) * group_probability[:, None]
    combine = jnp.einsum("sk,skc->sc", weights, placing, precision=lax.Precision.HIGHEST)
    dispatch = jnp.sum(placing, axis=1).astype(jnp.bfloat16)
    outgoing = jnp.einsum("sc,sd->cd", dispatch, normed_two, preferred_element_type=jnp.float32)
    outgoing = outgoing.astype(jnp.bfloat16).reshape(experts_all, capacity, model_width)
    width_local = expert_down_weight.shape[2]
    arrived = lax.all_to_all(outgoing, "ep", split_axis=0, concat_axis=0, tiled=True)
    held_slots = arrived.shape[1]
    grouped = arrived.reshape(ep_count, local_experts, held_slots, model_width)
    gate_pre = jnp.einsum(
        "sxcd,xfd->sxcf", grouped, expert_gate_weight, preferred_element_type=jnp.float32
    )
    up_pre = jnp.einsum(
        "sxcd,xfd->sxcf", grouped, expert_up_weight, preferred_element_type=jnp.float32
    )
    hidden = (jax.nn.silu(gate_pre) * up_pre).astype(jnp.bfloat16)
    outputs = jnp.einsum(
        "sxcf,xfd->sxcd",
        lax.all_gather(hidden, "tp", axis=3, tiled=True),
        expert_down_weight,
        preferred_element_type=jnp.float32,
    )
    ready_rows = outputs.astype(jnp.bfloat16).reshape(
        ep_count * local_experts, held_slots, width_local
    )
    returned = lax.all_to_all(ready_rows, "ep", split_axis=0, concat_axis=0, tiled=True)
    mixture = jnp.dot(
        combine,
        returned.reshape(slot_count, width_local).astype(jnp.float32),
        precision=lax.Precision.HIGHEST,
    )
    own_mixed = lax.dynamic_slice_in_dim(blended_tokens, tp_index * width_local, width_local, 1)
    new_stream = (own_mixed.astype(jnp.float32) + mixture).astype(jnp.bfloat16)
    return (new_stream, updated.reshape(seq_count, KEY_CHANNELS, value_local))


def greet(partners):
    barrier = pltpu.get_barrier_semaphore()
    for partner in partners:
        pl.semaphore_signal(barrier, inc=1, device_id=partner, device_id_type=MESH)
    pl.semaphore_wait(barrier, len(partners))


def send(source, target, send_sem, recv_sem, partner):
    copy = pltpu.make_async_remote_copy(
        src_ref=source,
        dst_ref=target,
        send_sem=send_sem,
        recv_sem=recv_sem,
        device_id=partner,
        device_id_type=MESH,
    )
    copy.start()
    return copy


def project_kernel(
    n,
    stream_ref,
    gain_ref,
    query_hbm,
    key_hbm,
    value_hbm,
    gate_hbm,
    lower_hbm,
    upper_hbm,
    boost_hbm,
    fkq_ref,
    value_ref,
    gate_ref,
    weights,
    lower,
    upper,
    boost,
    chunks,
    spread,
    pair_out,
    pair_in,
    own,
    plane_out,
    plane_in,
    load_sem,
    chunk_send,
    chunk_recv,
    pair_send,
    pair_recv,
    plane_send,
    plane_recv,
):
    me = lax.axis_index("ep")
    tp = lax.axis_index("tp")
    core = lax.rem(me, 2)
    row = me // 2
    rows = n // 2
    seqs = stream_ref.shape[0]
    feats = chunks.shape[2]
    span = boost.shape[1]
    width = value_hbm.shape[1]
    columns = pl.ds(pl.multiple_of(tp * span, 128), span)
    loads = [
        pltpu.make_async_copy(query_hbm.at[:, columns], weights.at[:, pl.ds(0, span)], load_sem.at[0]),
        pltpu.make_async_copy(key_hbm.at[:, columns], weights.at[:, pl.ds(span, span)], load_sem.at[1]),
        pltpu.make_async_copy(value_hbm, weights.at[:, pl.ds(2 * span, width)], load_sem.at[2]),
        pltpu.make_async_copy(gate_hbm, weights.at[:, pl.ds(2 * span + width, width)], load_sem.at[3]),
        pltpu.make_async_copy(lower_hbm, lower, load_sem.at[4]),
        pltpu.make_async_copy(upper_hbm.at[:, columns], upper, load_sem.at[5]),
        pltpu.make_async_copy(boost_hbm.at[:, columns], boost, load_sem.at[6]),
    ]
    for load in loads:
        load.start()
    floats = stream_ref[...].astype(F32)
    scale = lax.rsqrt(jnp.mean(floats * floats, axis=-1, keepdims=True) + epsilon)
    normed = (floats * scale * gain_ref[...]).astype(BF16)
    for d in range(n):
        chunks[d] = normed[:, d * feats : (d + 1) * feats]
    greet([{"ep": lax.rem(me + d, n)} for d in range(1, n)])
    sent = []
    for d in range(1, n):
        peer = lax.rem(me + d, n)
        slot = row + rows * (d % 2)
        sent.append(
            send(chunks.at[peer], spread.at[slot], chunk_send.at[d], chunk_recv.at[d], {"ep": peer})
        )
    spread[row] = chunks[me]
    for load in loads[4:]:
        load.wait()
    low_rank = jnp.dot(normed, lower[...], preferred_element_type=F32).astype(BF16)
    logit = jnp.dot(low_rank, upper[...], preferred_element_type=F32)
    log_sig = jnp.minimum(logit, 0.0) - jnp.log1p(jnp.exp(-jnp.abs(logit)))
    factor = jnp.exp(log_sig / forgetting_softness - boost[...])
    for load in loads[:4]:
        load.wait()
    for copy in sent:
        copy.wait_recv()
    half = rows * seqs
    x = spread[...].reshape(n * seqs, feats)
    cuts = [(0, 2 * span), (2 * span, width), (2 * span + width, width)]
    partner = {"ep": me + 1 - 2 * core}
    pairs = []
    for b, (start, size) in enumerate(cuts):
        part = jnp.dot(x, weights[:, start : start + size], preferred_element_type=F32)
        pair_out[:, start : start + size] = part[half:].astype(BF16)
        own[:, :, start : start + size] = part[:half].reshape(rows, seqs, size)
        at = (slice(None), pl.ds(start, size))
        pairs.append(
            send(pair_out.at[at], pair_in.at[at], pair_send.at[b], pair_recv.at[b], partner)
        )
    planes = []
    for b, (start, size) in enumerate(cuts):
        pairs[b].wait_recv()
        both = own[:, :, start : start + size] + pair_in[:, start : start + size].astype(
            F32
        ).reshape(rows, seqs, size)
        own[:, :, start : start + size] = both
        plane_out[:, :, start : start + size] = both.astype(BF16)
        for d in range(1, rows):
            there = lax.rem(row + d, rows)
            planes.append(
                send(
                    plane_out.at[there, :, pl.ds(start, size)],
                    plane_in.at[d, :, pl.ds(start, size)],
                    plane_send.at[b, d],
                    plane_recv.at[b, d],
                    {"ep": there * 2 + core},
                )
            )
    steps = seqs // STEP
    for b, (start, size) in enumerate(cuts):
        total = own[row, :, start : start + size]
        for d in range(1, rows):
            planes[b * (rows - 1) + d - 1].wait_recv()
            total = total + plane_in[d, :, start : start + size].astype(F32)
        if b == 0:
            query = (total[:, :span] * KEY_CHANNELS ** (-0.5)).astype(BF16).astype(F32)
            key = total[:, span:].astype(BF16).astype(F32)
            for i in range(steps):
                cut = slice(i * STEP, (i + 1) * STEP)
                fkq_ref[i, 0:STEP] = factor[cut]
                fkq_ref[i, STEP : 2 * STEP] = key[cut]
                fkq_ref[i, 2 * STEP : 3 * STEP] = query[cut]
                fkq_ref[i, 3 * STEP : 4 * STEP] = query[cut]
        else:
            target = value_ref if b == 1 else gate_ref
            total = total.astype(BF16).astype(F32)
            for i in range(steps):
                target[i] = total[i * STEP : (i + 1) * STEP]
    for copy in sent + pairs + planes:
        copy.wait_send()


def state_kernel(state_ref, fkq_ref, value_ref, gate_ref, gain_ref, out_ref, gated_ref):
    heads = value_ref.shape[2] // DV
    for h in range(heads):
        turned = fkq_ref[0, :, h * KEY_CHANNELS : (h + 1) * KEY_CHANNELS].T
        lanes = slice(h * DV, (h + 1) * DV)
        for s in range(STEP):
            factor = turned[:, s : s + 1]
            key = turned[:, STEP + s : STEP + s + 1]
            query = turned[:, 2 * STEP + s : 2 * STEP + s + 1]
            updated = factor * state_ref[s, :, lanes] + key * value_ref[0, s : s + 1, lanes]
            out_ref[s, :, lanes] = updated
            readout = jnp.sum(query * updated, axis=0, keepdims=True)
            mean_sq = jnp.mean(readout * readout, axis=-1, keepdims=True)
            gate = gate_ref[0, s : s + 1, lanes]
            silu = gate / (1.0 + jnp.exp(-gate))
            gated_ref[0, s : s + 1, lanes] = (
                readout * lax.rsqrt(mean_sq + epsilon) * gain_ref[...] * silu
            )


def mixture_kernel(
    n,
    m,
    gated_ref,
    stream_hbm,
    gain_ref,
    index_ref,
    score_ref,
    prob_ref,
    output_hbm,
    gate_hbm,
    up_hbm,
    down_hbm,
    out_ref,
    own_stream,
    w_out,
    w_gate,
    w_up,
    w_down,
    lhs,
    part_out,
    part_in,
    slots_out,
    arrived,
    hidden,
    ready,
    returned,
    load_sem,
    part_send,
    part_recv,
    slot_send,
    slot_recv,
    join_send,
    join_recv,
    hid_send,
    hid_recv,
    back_send,
    back_recv,
):
    me = lax.axis_index("ep")
    tp = lax.axis_index("tp")
    seqs, width = own_stream.shape
    capacity = arrived.shape[2]
    others = [lax.rem(tp + d, m) for d in range(1, m)] + [tp]
    loads = []
    for j, there in enumerate(others):
        cut = pl.ds(pl.multiple_of(there * width, 128), width)
        loads.append(pltpu.make_async_copy(output_hbm.at[:, cut], w_out.at[j], load_sem.at[j]))
    own_cut = pl.ds(pl.multiple_of(tp * width, 128), width)
    loads += [
        pltpu.make_async_copy(stream_hbm.at[:, own_cut], own_stream, load_sem.at[m]),
        pltpu.make_async_copy(gate_hbm.at[0], w_gate, load_sem.at[m + 1]),
        pltpu.make_async_copy(up_hbm.at[0], w_up, load_sem.at[m + 2]),
        pltpu.make_async_copy(down_hbm.at[0], w_down, load_sem.at[m + 3]),
    ]
    for load in loads:
        load.start()
    for i in range(seqs // STEP):
        lhs[i * STEP : (i + 1) * STEP] = gated_ref[i]
    gated = lhs[...].astype(BF16)
    greet(
        [{"tp": there} for there in others[:-1]]
        + [{"ep": lax.rem(me + d, n)} for d in range(1, n)]
    )
    parts = []
    for j, there in enumerate(others):
        loads[j].wait()
        part = jnp.dot(gated, w_out[j], preferred_element_type=F32)
        if j < m - 1:
            part_out[j] = part.astype(BF16)
            parts.append(
                send(part_out.at[j], part_in.at[j], part_send.at[j], part_recv.at[j], {"tp": there})
            )

    index = index_ref[...]
    group = index[:, 0:1] // (n // GROUPS)
    lane = lax.broadcasted_iota(jnp.int32, (seqs, 128), 1)
    one_hot = (lane == group).astype(F32)
    earlier = lax.broadcasted_iota(jnp.int32, (seqs, seqs), 1) < lax.broadcasted_iota(
        jnp.int32, (seqs, seqs), 0
    )
    counts = jnp.dot(earlier.astype(F32), one_hot, preferred_element_type=F32)
    rank = jnp.sum(counts * one_hot, axis=1, keepdims=True).astype(jnp.int32)
    slot_lane = lax.broadcasted_iota(jnp.int32, (seqs, GROUPS * capacity), 1)
    placing = (slot_lane == group * capacity + rank).astype(F32)
    scores = jnp.exp(score_ref[...])
    weights = scores / jnp.sum(scores, axis=-1, keepdims=True) * prob_ref[...]
    back_lane = lax.broadcasted_iota(jnp.int32, (seqs, n * capacity), 1)
    combine = jnp.zeros((seqs, n * capacity), F32)
    for k in range(index.shape[1]):
        combine += jnp.where(
            back_lane == index[:, k : k + 1] * capacity + rank, weights[:, k : k + 1], 0.0
        )

    loads[m].wait()
    total = part
    for j in range(m - 1):
        parts[j].wait_recv()
        total = total + part_in[j].astype(F32)
    mixed = (own_stream[...].astype(F32) + total).astype(BF16)
    slots = lax.dot_general(
        placing, mixed.astype(F32), (((0,), (0,)), ((), ())), preferred_element_type=F32
    )
    slots_out[...] = slots.reshape(GROUPS, capacity, width).astype(BF16)
    moved = []
    per = n // GROUPS
    for d in range(1, n):
        peer = lax.rem(me + d, n)
        moved.append(
            send(
                slots_out.at[peer // per],
                arrived.at[tp, me],
                slot_send.at[d],
                slot_recv.at[d],
                {"ep": peer},
            )
        )
    arrived[tp, me] = slots_out[me // per]
    for copy in moved:
        copy.wait_recv()
    joins = []
    for j, there in enumerate(others[:-1]):
        joins.append(
            send(arrived.at[tp], arrived.at[tp], join_send.at[j], join_recv.at[j], {"tp": there})
        )
    for copy in joins:
        copy.wait_recv()
    square = jnp.zeros((n * capacity, 1), F32)
    for t in range(m):
        tokens = arrived[t].astype(F32).reshape(n * capacity, width)
        square += jnp.sum(tokens * tokens, axis=-1, keepdims=True)
    scale = lax.rsqrt(square / (m * width) + epsilon)
    for load in loads[m + 1 : m + 3]:
        load.wait()
    nt = (((1,), (1,)), ((), ()))
    gate_pre = jnp.zeros((n * capacity, w_gate.shape[0]), F32)
    up_pre = jnp.zeros((n * capacity, w_gate.shape[0]), F32)
    for t in range(m):
        cut = slice(t * width, (t + 1) * width)
        tokens = arrived[t].astype(F32).reshape(n * capacity, width)
        normed = (tokens * scale * gain_ref[:, cut]).astype(BF16)
        gate_pre += lax.dot_general(normed, w_gate[:, cut], nt, preferred_element_type=F32)
        up_pre += lax.dot_general(normed, w_up[:, cut], nt, preferred_element_type=F32)
    inner = gate_pre.shape[1]
    hidden[tp] = (gate_pre / (1.0 + jnp.exp(-gate_pre)) * up_pre).astype(BF16)
    shared = []
    for j, there in enumerate(others[:-1]):
        shared.append(
            send(hidden.at[tp], hidden.at[tp], hid_send.at[j], hid_recv.at[j], {"tp": there})
        )
    loads[m + 3].wait()
    for copy in shared:
        copy.wait_recv()
    outputs = jnp.zeros((n * capacity, width), F32)
    for t in range(m):
        outputs += jnp.dot(
            hidden[t], w_down[t * inner : (t + 1) * inner, :], preferred_element_type=F32
        )
    ready[...] = outputs.reshape(n, capacity, width).astype(BF16)
    backs = []
    for d in range(1, n):
        peer = lax.rem(me + d, n)
        backs.append(
            send(ready.at[peer], returned.at[me], back_send.at[d], back_recv.at[d], {"ep": peer})
        )
    returned[me] = ready[me]
    for copy in backs:
        copy.wait_recv()
    rows = returned[...].astype(F32).reshape(n * capacity, width)
    mixture = jnp.dot(
        combine, rows, preferred_element_type=F32, precision=lax.Precision.HIGHEST
    )
    out_ref[...] = (mixed.astype(F32) + mixture).astype(BF16)
    for copy in parts + moved + joins + shared + backs:
        copy.wait_send()


def fused(
    stream,
    previous_state,
    mixer_norm_gain,
    query_matrix,
    key_matrix,
    value_matrix,
    output_gate_weight,
    decay_lower_factor,
    decay_upper_factor,
    forgetting_boost,
    head_norm_gain,
    output_matrix,
    mixture_norm_gain,
    expert_gate_weight,
    expert_up_weight,
    expert_down_weight,
    expert_index_table,
    expert_scores_within,
    group_probability,
):
    n = lax.axis_size("ep")
    m = lax.axis_size("tp")
    seqs, model = stream.shape
    width = previous_state.shape[2]
    span = width // DV * KEY_CHANNELS
    feats = query_matrix.shape[0]
    rank = decay_lower_factor.shape[1]
    steps = seqs // STEP
    total = 2 * span + 2 * width
    rows = n // 2
    half = rows * seqs
    dma = pltpu.SemaphoreType.DMA
    vmem = pl.BlockSpec(memory_space=pltpu.VMEM)
    hbm = pl.BlockSpec(memory_space=pl.ANY)
    fkq, values, gates = pl.pallas_call(
        functools.partial(project_kernel, n),
        name="project",
        out_shape=(
            jax.ShapeDtypeStruct((steps, 4 * STEP, span), F32),
            jax.ShapeDtypeStruct((steps, STEP, width), F32),
            jax.ShapeDtypeStruct((steps, STEP, width), F32),
        ),
        in_specs=[vmem, vmem] + [hbm] * 7,
        out_specs=(vmem, vmem, vmem),
        scratch_shapes=[
            pltpu.VMEM((feats, total), BF16),
            pltpu.VMEM((model, rank), BF16),
            pltpu.VMEM((rank, span), BF16),
            pltpu.VMEM((seqs, span), F32),
            pltpu.VMEM((n, seqs, feats), BF16),
            pltpu.VMEM((n, seqs, feats), BF16),
            pltpu.VMEM((half, total), BF16),
            pltpu.VMEM((half, total), BF16),
            pltpu.VMEM((rows, seqs, total), F32),
            pltpu.VMEM((rows, seqs, total), BF16),
            pltpu.VMEM((rows, seqs, total), BF16),
            dma((7,)),
            dma((n,)),
            dma((n,)),
            dma((3,)),
            dma((3,)),
            dma((3, rows)),
            dma((3, rows)),
        ],
        compiler_params=pltpu.CompilerParams(
            collective_id=0, has_side_effects=True, vmem_limit_bytes=24 * 2**20
        ),
    )(
        stream,
        mixer_norm_gain.reshape(1, model),
        query_matrix,
        key_matrix,
        value_matrix,
        output_gate_weight,
        decay_lower_factor,
        decay_upper_factor,
        forgetting_boost,
    )
    state_block = pl.BlockSpec((STEP, KEY_CHANNELS, width), lambda i: (i, 0, 0))
    row_block = pl.BlockSpec((1, STEP, width), lambda i: (i, 0, 0))
    new_state, gated = pl.pallas_call(
        state_kernel,
        name="state",
        grid=(steps,),
        out_shape=(
            jax.ShapeDtypeStruct(previous_state.shape, F32),
            jax.ShapeDtypeStruct((steps, STEP, width), F32),
        ),
        in_specs=[
            state_block,
            pl.BlockSpec((1, 4 * STEP, span), lambda i: (i, 0, 0)),
            row_block,
            row_block,
            pl.BlockSpec((1, DV), lambda i: (0, 0)),
        ],
        out_specs=(state_block, row_block),
        compiler_params=pltpu.CompilerParams(
            dimension_semantics=("arbitrary",), vmem_limit_bytes=24 * 2**20
        ),
    )(previous_state, fkq, values, gates, head_norm_gain.reshape(1, DV))
    inner = expert_gate_weight.shape[1]
    deep = expert_down_weight.shape[1]
    capacity = 2 * seqs * expert_index_table.shape[1] // n
    new_stream = pl.pallas_call(
        functools.partial(mixture_kernel, n, m),
        name="mixture",
        out_shape=jax.ShapeDtypeStruct((seqs, width), BF16),
        in_specs=[vmem, hbm, vmem, vmem, vmem, vmem, hbm, hbm, hbm, hbm],
        out_specs=vmem,
        scratch_shapes=[
            pltpu.VMEM((seqs, width), BF16),
            pltpu.VMEM((m, width, width), BF16),
            pltpu.VMEM((inner, model), BF16),
            pltpu.VMEM((inner, model), BF16),
            pltpu.VMEM((deep, width), BF16),
            pltpu.VMEM((seqs, width), F32),
            pltpu.VMEM((m - 1, seqs, width), BF16),
            pltpu.VMEM((m - 1, seqs, width), BF16),
            pltpu.VMEM((GROUPS, capacity, width), BF16),
            pltpu.VMEM((m, n, capacity, width), BF16),
            pltpu.VMEM((m, n * capacity, inner), BF16),
            pltpu.VMEM((n, capacity, width), BF16),
            pltpu.VMEM((n, capacity, width), BF16),
            dma((m + 4,)),
            dma((m - 1,)),
            dma((m - 1,)),
            dma((n,)),
            dma((n,)),
            dma((m - 1,)),
            dma((m - 1,)),
            dma((m - 1,)),
            dma((m - 1,)),
            dma((n,)),
            dma((n,)),
        ],
        compiler_params=pltpu.CompilerParams(
            collective_id=1, has_side_effects=True, vmem_limit_bytes=32 * 2**20
        ),
    )(
        gated,
        stream,
        mixture_norm_gain.reshape(1, model),
        expert_index_table,
        expert_scores_within,
        group_probability.reshape(seqs, 1),
        output_matrix,
        expert_gate_weight,
        expert_up_weight,
        expert_down_weight,
    )
    return (new_stream, new_state)


def on_device(*arrays):
    stream, state = arrays[0], arrays[1]
    experts_held, route_count = arrays[13].shape[0], arrays[16].shape[1]
    n = lax.axis_size("ep")
    whole_heads = state.shape[2] % DV == 0
    pair_routed = experts_held == 1 and n == GROUPS * route_count and route_count == 2
    full_tiles = stream.shape[0] % 16 == 0 and stream.shape[1] == state.shape[2] * lax.axis_size("tp")
    if whole_heads and pair_routed and full_tiles:
        return fused(*arrays)
    return general(*arrays)


def solution(mesh):
    placed = (
        P("ep", None),
        P("ep", None, "tp"),
        P(),
        P("ep", None),
        P("ep", None),
        P("ep", "tp"),
        P("ep", "tp"),
        P(),
        P(),
        P("ep", None),
        P(),
        P("tp", None),
        P(),
        P("ep", "tp", None),
        P("ep", "tp", None),
        P("ep", None, "tp"),
        P("ep", None),
        P("ep", None),
        P("ep"),
    )
    return jax.shard_map(
        on_device,
        mesh=mesh,
        in_specs=placed,
        out_specs=(P("ep", "tp"), P("ep", None, "tp")),
        check_vma=False,
    )
```

```python
import functools

import jax
import jax.numpy as jnp
from jax import lax
from jax.experimental import pallas as pl
from jax.experimental.pallas import tpu as pltpu
from jax.sharding import PartitionSpec as P

HEAD_TOTAL = 16
KEY_CHANNELS = 128
DV = 256
GROUPS = 4
STEP = 2
COST = 20_000_000_000
VM3 = 24
F32 = jnp.float32
BF16 = jnp.bfloat16
MESH = pl.DeviceIdType.MESH

epsilon = 1e-06
forgetting_softness = 16.0


def rms_scaled(values, gain_vec):
    floats = values.astype(jnp.float32)
    scaled = floats * lax.rsqrt(jnp.mean(floats * floats, axis=-1, keepdims=True) + epsilon)
    return (scaled * gain_vec).astype(jnp.bfloat16)


def general(
    stream,
    previous_state,
    mixer_norm_gain,
    query_matrix,
    key_matrix,
    value_matrix,
    output_gate_weight,
    decay_lower_factor,
    decay_upper_factor,
    forgetting_boost,
    head_norm_gain,
    output_matrix,
    mixture_norm_gain,
    expert_gate_weight,
    expert_up_weight,
    expert_down_weight,
    expert_index_table,
    expert_scores_within,
    group_probability,
):
    seq_count, model_width = stream.shape
    value_local = previous_state.shape[2]
    head_count = max(1, value_local // DV)
    head_width = min(value_local, DV)
    tp_index = lax.axis_index("tp")
    leading_head = tp_index * value_local // DV
    value_start = tp_index * value_local % DV
    key_column_span = head_count * KEY_CHANNELS
    normed = rms_scaled(stream, mixer_norm_gain)
    own_query = lax.dynamic_slice_in_dim(
        query_matrix, leading_head * KEY_CHANNELS, key_column_span, 1
    )
    own_key = lax.dynamic_slice_in_dim(key_matrix, leading_head * KEY_CHANNELS, key_column_span, 1)
    spread = lax.all_to_all(normed, "ep", split_axis=1, concat_axis=0, tiled=True)
    joined = jnp.concatenate([own_query, own_key, value_matrix, output_gate_weight], axis=1)
    summed = lax.psum_scatter(
        jnp.dot(spread, joined, preferred_element_type=jnp.float32),
        "ep",
        scatter_dimension=0,
        tiled=True,
    )
    query_sum = summed[:, :key_column_span]
    key_sum = summed[:, key_column_span : 2 * key_column_span]
    value_sum = summed[:, 2 * key_column_span : 2 * key_column_span + value_local]
    gate_sum = summed[:, 2 * key_column_span + value_local :]
    queries = (query_sum * KEY_CHANNELS ** (-0.5)).astype(jnp.bfloat16)
    key_rows = key_sum.astype(jnp.bfloat16)
    value_rows = value_sum.astype(jnp.bfloat16)
    gate_rows = gate_sum.astype(jnp.bfloat16)
    low_rank = jnp.dot(normed, decay_lower_factor, preferred_element_type=jnp.float32).astype(
        jnp.bfloat16
    )
    local_expand_matrix = lax.dynamic_slice_in_dim(
        decay_upper_factor, leading_head * KEY_CHANNELS, key_column_span, 1
    )
    forgetting_logit = jnp.dot(low_rank, local_expand_matrix, preferred_element_type=jnp.float32)
    request_boost = lax.dynamic_slice_in_dim(
        forgetting_boost, leading_head * KEY_CHANNELS, key_column_span, 1
    )
    forgetting_lograte = jax.nn.log_sigmoid(forgetting_logit) / forgetting_softness - request_boost
    factor = (
        jnp.exp(forgetting_lograte)
        .reshape(seq_count, head_count, KEY_CHANNELS)
        .transpose(0, 2, 1)[..., None]
    )
    state_four = previous_state.reshape(seq_count, KEY_CHANNELS, head_count, head_width)
    key_part = (
        key_rows.astype(jnp.float32)
        .reshape(seq_count, head_count, KEY_CHANNELS)
        .transpose(0, 2, 1)[..., None]
    )
    value_part = value_rows.astype(jnp.float32).reshape(seq_count, 1, head_count, head_width)
    updated = factor * state_four + key_part * value_part
    query_part = (
        queries.astype(jnp.float32).reshape(seq_count, head_count, KEY_CHANNELS).transpose(0, 2, 1)
    )
    readout = jnp.einsum("skh,skhv->shv", query_part, updated, precision=lax.Precision.HIGHEST)
    square_sums = jnp.sum(readout * readout, axis=-1)
    norm_table = lax.dynamic_update_slice(
        jnp.zeros((seq_count, HEAD_TOTAL), jnp.float32), square_sums, (jnp.int32(0), leading_head)
    )
    totals = lax.psum(norm_table, "tp")
    own_totals = lax.dynamic_slice_in_dim(totals, leading_head, head_count, 1)
    mean_sq = own_totals[..., None] / DV
    own_gain = lax.dynamic_slice_in_dim(head_norm_gain, value_start, head_width, 0)
    gate_part = jax.nn.silu(
        gate_rows.astype(jnp.float32).reshape(seq_count, head_count, head_width)
    )
    gated_rows = (
        (readout * lax.rsqrt(mean_sq + epsilon) * own_gain * gate_part)
        .reshape(seq_count, value_local)
        .astype(jnp.bfloat16)
    )
    partial_out = jnp.dot(gated_rows, output_matrix, preferred_element_type=jnp.float32)
    mixer_sum = lax.psum(partial_out.astype(jnp.bfloat16), "tp").astype(jnp.float32)
    blended_tokens = (stream.astype(jnp.float32) + mixer_sum).astype(jnp.bfloat16)
    normed_two = rms_scaled(blended_tokens, mixture_norm_gain)
    ep_count = lax.axis_size("ep")
    local_experts = expert_gate_weight.shape[0]
    experts_all = ep_count * local_experts
    route_count = expert_index_table.shape[1]
    capacity = 2 * seq_count * route_count // experts_all
    slot_count = experts_all * capacity
    flat_ids = expert_index_table.reshape(seq_count * route_count)
    one_hot = (flat_ids[:, None] == jnp.arange(experts_all, dtype=jnp.int32)[None, :]).astype(
        jnp.int32
    )
    rank_in = jnp.sum(one_hot * (jnp.cumsum(one_hot, axis=0) - 1), axis=1)
    place_lookup = flat_ids * capacity + rank_in
    placing = (place_lookup[:, None] == jnp.arange(slot_count, dtype=jnp.int32)[None, :]).astype(
        jnp.float32
    )
    placing = placing.reshape(seq_count, route_count, slot_count)
    logit_exp = jnp.exp(expert_scores_within)
    weights = logit_exp / jnp.sum(logit_exp, axis=-1, keepdims=True) * group_probability[:, None]
    combine = jnp.einsum("sk,skc->sc", weights, placing, precision=lax.Precision.HIGHEST)
    dispatch = jnp.sum(placing, axis=1).astype(jnp.bfloat16)
    outgoing = jnp.einsum("sc,sd->cd", dispatch, normed_two, preferred_element_type=jnp.float32)
    outgoing = outgoing.astype(jnp.bfloat16).reshape(experts_all, capacity, model_width)
    width_local = expert_down_weight.shape[2]
    arrived = lax.all_to_all(outgoing, "ep", split_axis=0, concat_axis=0, tiled=True)
    held_slots = arrived.shape[1]
    grouped = arrived.reshape(ep_count, local_experts, held_slots, model_width)
    gate_pre = jnp.einsum(
        "sxcd,xfd->sxcf", grouped, expert_gate_weight, preferred_element_type=jnp.float32
    )
    up_pre = jnp.einsum(
        "sxcd,xfd->sxcf", grouped, expert_up_weight, preferred_element_type=jnp.float32
    )
    hidden = (jax.nn.silu(gate_pre) * up_pre).astype(jnp.bfloat16)
    outputs = jnp.einsum(
        "sxcf,xfd->sxcd",
        lax.all_gather(hidden, "tp", axis=3, tiled=True),
        expert_down_weight,
        preferred_element_type=jnp.float32,
    )
    ready_rows = outputs.astype(jnp.bfloat16).reshape(
        ep_count * local_experts, held_slots, width_local
    )
    returned = lax.all_to_all(ready_rows, "ep", split_axis=0, concat_axis=0, tiled=True)
    mixture = jnp.dot(
        combine,
        returned.reshape(slot_count, width_local).astype(jnp.float32),
        precision=lax.Precision.HIGHEST,
    )
    own_mixed = lax.dynamic_slice_in_dim(blended_tokens, tp_index * width_local, width_local, 1)
    new_stream = (own_mixed.astype(jnp.float32) + mixture).astype(jnp.bfloat16)
    return (new_stream, updated.reshape(seq_count, KEY_CHANNELS, value_local))


def greet(partners):
    barrier = pltpu.get_barrier_semaphore()
    for partner in partners:
        pl.semaphore_signal(barrier, inc=1, device_id=partner, device_id_type=MESH)
    pl.semaphore_wait(barrier, len(partners))


def send(source, target, send_sem, recv_sem, partner):
    copy = pltpu.make_async_remote_copy(
        src_ref=source,
        dst_ref=target,
        send_sem=send_sem,
        recv_sem=recv_sem,
        device_id=partner,
        device_id_type=MESH,
    )
    copy.start()
    return copy


def project_kernel(
    n,
    stream_hbm,
    gain_hbm,
    query_hbm,
    key_hbm,
    value_hbm,
    gate_hbm,
    lower_hbm,
    upper_hbm,
    boost_hbm,
    fkq_ref,
    value_ref,
    gate_ref,
    stream,
    gain,
    weights,
    lower,
    upper,
    boost,
    chunks,
    spread,
    pair_out,
    pair_in,
    own,
    plane_out,
    plane_in,
    load_sem,
    chunk_send,
    chunk_recv,
    pair_send,
    pair_recv,
    plane_send,
    plane_recv,
):
    me = lax.axis_index("ep")
    tp = lax.axis_index("tp")
    core = lax.rem(me, 2)
    row = me // 2
    rows = n // 2
    seqs = stream.shape[0]
    feats = chunks.shape[2]
    span = boost.shape[1]
    width = value_hbm.shape[1]
    columns = pl.ds(pl.multiple_of(tp * span, 128), span)
    loads = [
        pltpu.make_async_copy(query_hbm.at[:, columns], weights.at[:, pl.ds(0, span)], load_sem.at[0]),
        pltpu.make_async_copy(key_hbm.at[:, columns], weights.at[:, pl.ds(span, span)], load_sem.at[1]),
        pltpu.make_async_copy(value_hbm, weights.at[:, pl.ds(2 * span, width)], load_sem.at[2]),
        pltpu.make_async_copy(gate_hbm, weights.at[:, pl.ds(2 * span + width, width)], load_sem.at[3]),
        pltpu.make_async_copy(lower_hbm, lower, load_sem.at[4]),
        pltpu.make_async_copy(upper_hbm.at[:, columns], upper, load_sem.at[5]),
        pltpu.make_async_copy(boost_hbm.at[:, columns], boost, load_sem.at[6]),
    ]
    first = [
        pltpu.make_async_copy(stream_hbm, stream, load_sem.at[7]),
        pltpu.make_async_copy(gain_hbm, gain, load_sem.at[8]),
    ]
    for load in first + loads:
        load.start()
    greet([{"ep": lax.rem(me + d, n)} for d in range(1, n)])
    for load in first:
        load.wait()
    floats = stream[...].astype(F32)
    scale = lax.rsqrt(jnp.mean(floats * floats, axis=-1, keepdims=True) + epsilon)
    normed = (floats * scale * gain[...]).astype(BF16)
    for d in range(n):
        chunks[d] = normed[:, d * feats : (d + 1) * feats]
    sent = []
    for d in range(1, n):
        peer = lax.rem(me + d, n)
        slot = row + rows * (d % 2)
        sent.append(
            send(chunks.at[peer], spread.at[slot], chunk_send.at[d], chunk_recv.at[d], {"ep": peer})
        )
    spread[row] = chunks[me]
    for load in loads[4:]:
        load.wait()
    nt = (((1,), (1,)), ((), ()))
    low_rank = lax.dot_general(normed, lower[...], nt, preferred_element_type=F32).astype(BF16)
    logit = jnp.dot(low_rank, upper[...], preferred_element_type=F32)
    log_sig = jnp.minimum(logit, 0.0) - jnp.log1p(jnp.exp(-jnp.abs(logit)))
    factor = jnp.exp(log_sig / forgetting_softness - boost[...])
    for load in loads[:4]:
        load.wait()
    for copy in sent:
        copy.wait_recv()
    half = rows * seqs
    x = spread[...].reshape(n * seqs, feats)
    cuts = [(0, 2 * span), (2 * span, width), (2 * span + width, width)]
    partner = {"ep": me + 1 - 2 * core}
    pairs = []
    for b, (start, size) in enumerate(cuts):
        part = jnp.dot(x, weights[:, start : start + size], preferred_element_type=F32)
        pair_out[:, start : start + size] = part[half:].astype(BF16)
        own[:, :, start : start + size] = part[:half].reshape(rows, seqs, size)
        at = (slice(None), pl.ds(start, size))
        pairs.append(
            send(pair_out.at[at], pair_in.at[at], pair_send.at[b], pair_recv.at[b], partner)
        )
    planes = []
    for b, (start, size) in enumerate(cuts):
        pairs[b].wait_recv()
        both = own[:, :, start : start + size] + pair_in[:, start : start + size].astype(
            F32
        ).reshape(rows, seqs, size)
        own[:, :, start : start + size] = both
        plane_out[:, :, start : start + size] = both.astype(BF16)
        for d in range(1, rows):
            there = lax.rem(row + d, rows)
            planes.append(
                send(
                    plane_out.at[there, :, pl.ds(start, size)],
                    plane_in.at[d, :, pl.ds(start, size)],
                    plane_send.at[b, d],
                    plane_recv.at[b, d],
                    {"ep": there * 2 + core},
                )
            )
    steps = seqs // STEP
    for b, (start, size) in enumerate(cuts):
        total = own[row, :, start : start + size]
        for d in range(1, rows):
            planes[b * (rows - 1) + d - 1].wait_recv()
            total = total + plane_in[d, :, start : start + size].astype(F32)
        if b == 0:
            query = (total[:, :span] * KEY_CHANNELS ** (-0.5)).astype(BF16).astype(F32)
            key = total[:, span:].astype(BF16).astype(F32)
            for i in range(steps):
                cut = slice(i * STEP, (i + 1) * STEP)
                fkq_ref[i, 0:STEP] = factor[cut]
                fkq_ref[i, STEP : 2 * STEP] = key[cut]
                fkq_ref[i, 2 * STEP : 3 * STEP] = query[cut]
                fkq_ref[i, 3 * STEP : 4 * STEP] = query[cut]
        else:
            target = value_ref if b == 1 else gate_ref
            total = total.astype(BF16).astype(F32)
            for i in range(steps):
                target[i] = total[i * STEP : (i + 1) * STEP]
    for copy in sent + pairs + planes:
        copy.wait_send()


def state_kernel(state_ref, fkq_ref, value_ref, new_hbm, read_ref, turned, buffer, out_sem):
    seqs, _, width = state_ref.shape
    heads = width // DV
    steps = seqs // STEP

    def flush(i, slot):
        return pltpu.make_async_copy(
            buffer.at[slot], new_hbm.at[pl.ds(i * STEP, STEP)], out_sem.at[slot]
        )

    @pl.loop(0, steps)
    def _(i):
        slot = lax.rem(i, 2)

        @pl.when(i >= 2)
        def _():
            flush(i - 2, slot).wait()

        for h in range(heads):
            turned[h] = fkq_ref[i, :, h * KEY_CHANNELS : (h + 1) * KEY_CHANNELS].T
        for s in range(STEP):
            sums = []
            for h in range(heads):
                lanes = slice(h * DV, (h + 1) * DV)
                factor = turned[h, :, s : s + 1]
                key = turned[h, :, STEP + s : STEP + s + 1]
                query = turned[h, :, 2 * STEP + s : 2 * STEP + s + 1]
                updated = factor * state_ref[i * STEP + s, :, lanes] + key * value_ref[
                    i, s : s + 1, lanes
                ]
                buffer[slot, s, :, lanes] = updated
                sums.append(jnp.sum((query * updated).reshape(-1, 8, DV), axis=0))
            read_ref[i * STEP + s] = jnp.concatenate(sums, axis=1)
        flush(i, slot).start()

    for i in range(steps - 2, steps):
        flush(i, i % 2).wait()


def mixture_kernel(
    n,
    m,
    read_ref,
    rows_ref,
    head_gain_ref,
    stream_hbm,
    gain_ref,
    index_ref,
    score_ref,
    prob_ref,
    output_hbm,
    gate_hbm,
    up_hbm,
    down_hbm,
    out_ref,
    own_stream,
    w_out,
    w_gate,
    w_up,
    w_down,
    lhs,
    part_out,
    part_in,
    slots_out,
    arrived,
    hidden,
    ready,
    returned,
    load_sem,
    part_send,
    part_recv,
    slot_send,
    slot_recv,
    join_send,
    join_recv,
    swap_send,
    swap_recv,
    hid_send,
    hid_recv,
    back_send,
    back_recv,
):
    me = lax.axis_index("ep")
    tp = lax.axis_index("tp")
    seqs, width = own_stream.shape
    rows = n // 2
    capacity = slots_out.shape[1]
    others = [lax.rem(tp + d, m) for d in range(1, m)] + [tp]
    own_cut = pl.ds(pl.multiple_of(tp * width, 128), width)
    load = pltpu.make_async_copy(stream_hbm.at[:, own_cut], own_stream, load_sem.at[m + 3])
    loads = []
    for j, there in enumerate(others):
        cut = pl.ds(pl.multiple_of(there * width, 128), width)
        loads.append(pltpu.make_async_copy(output_hbm.at[:, cut], w_out.at[j], load_sem.at[j]))
    loads += [
        pltpu.make_async_copy(gate_hbm, w_gate, load_sem.at[m]),
        pltpu.make_async_copy(up_hbm, w_up, load_sem.at[m + 1]),
        pltpu.make_async_copy(down_hbm, w_down, load_sem.at[m + 2]),
    ]
    for one in loads + [load]:
        one.start()
    for i in range(seqs // STEP):
        lhs[i * STEP : (i + 1) * STEP] = rows_ref[i]
    gates = lhs[...]
    silu = gates / (1.0 + jnp.exp(-gates))
    readout = jnp.sum(read_ref[...], axis=1)
    for h in range(width // DV):
        lanes = slice(h * DV, (h + 1) * DV)
        part = readout[:, lanes]
        mean_sq = jnp.mean(part * part, axis=-1, keepdims=True)
        lhs[:, lanes] = part * lax.rsqrt(mean_sq + epsilon) * head_gain_ref[...] * silu[:, lanes]
    gated = lhs[...].astype(BF16)
    greet(
        [{"tp": there} for there in others[:-1]]
        + [{"ep": lax.rem(me + d, n)} for d in range(1, n)]
    )
    parts = []
    for j, there in enumerate(others):
        loads[j].wait()
        part = jnp.dot(gated, w_out[j], preferred_element_type=F32)
        if j < m - 1:
            part_out[j] = part.astype(BF16)
            parts.append(
                send(part_out.at[j], part_in.at[j], part_send.at[j], part_recv.at[j], {"tp": there})
            )

    index = index_ref[...]
    group = index[:, 0:1] // (n // GROUPS)
    lane = lax.broadcasted_iota(jnp.int32, (seqs, 128), 1)
    one_hot = (lane == group).astype(F32)
    earlier = lax.broadcasted_iota(jnp.int32, (seqs, seqs), 1) < lax.broadcasted_iota(
        jnp.int32, (seqs, seqs), 0
    )
    counts = jnp.dot(earlier.astype(F32), one_hot, preferred_element_type=F32)
    rank = jnp.sum(counts * one_hot, axis=1, keepdims=True).astype(jnp.int32)
    slot_lane = lax.broadcasted_iota(jnp.int32, (seqs, GROUPS * capacity), 1)
    placing = (slot_lane == group * capacity + rank).astype(F32)
    scores = jnp.exp(score_ref[...])
    weights = scores / jnp.sum(scores, axis=-1, keepdims=True) * prob_ref[...]
    back_lane = lax.broadcasted_iota(jnp.int32, (seqs, n * capacity), 1)
    combine = jnp.zeros((seqs, n * capacity), F32)
    for k in range(index.shape[1]):
        combine += jnp.where(
            back_lane == index[:, k : k + 1] * capacity + rank, weights[:, k : k + 1], 0.0
        )

    load.wait()
    total = part
    for j in range(m - 1):
        parts[j].wait_recv()
        total = total + part_in[j].astype(F32)
    mixed = (own_stream[...].astype(F32) + total).astype(BF16)
    slots = lax.dot_general(
        placing, mixed.astype(F32), (((0,), (0,)), ((), ())), preferred_element_type=F32
    )
    slots_out[...] = slots.reshape(GROUPS, capacity, width).astype(BF16)
    core = lax.rem(me, 2)
    row = me // 2
    moved = []
    for d in range(1, rows):
        there = lax.rem(row + d, rows)
        moved.append(
            send(
                slots_out.at[there],
                arrived.at[tp, core, row],
                slot_send.at[d],
                slot_recv.at[d],
                {"ep": there * 2 + core},
            )
        )
    arrived[tp, core, row] = slots_out[row]
    for copy in moved:
        copy.wait_recv()
    joins = []
    for j, there in enumerate(others[:-1]):
        joins.append(
            send(
                arrived.at[tp, core],
                arrived.at[tp, core],
                join_send.at[j],
                join_recv.at[j],
                {"tp": there},
            )
        )
    for one in loads[m:]:
        one.wait()
    swaps = []
    nt = (((1,), (1,)), ((), ()))
    tokens_held = n * capacity
    square = jnp.zeros((tokens_held, 1), F32)
    gate_pre = jnp.zeros((tokens_held, w_gate.shape[1]), F32)
    up_pre = jnp.zeros((tokens_held, w_gate.shape[1]), F32)
    origin = [tp] + [lax.rem(tp - 1 - j + m, m) for j in range(m - 1)]
    for j, t in enumerate(origin):
        if j > 0:
            joins[j - 1].wait_recv()
        swaps.append(
            send(
                arrived.at[t, core],
                arrived.at[t, core],
                swap_send.at[j],
                swap_recv.at[j],
                {"ep": me + 1 - 2 * core},
            )
        )
    for j, t in enumerate(origin):
        swaps[j].wait_recv()
        cut = pl.ds(pl.multiple_of(t * width, 128), width)
        tokens = arrived[t].astype(F32).reshape(tokens_held, width)
        square += jnp.sum(tokens * tokens, axis=-1, keepdims=True)
        scaled = (tokens * gain_ref[:, cut]).astype(BF16)
        gate_pre += lax.dot_general(scaled, w_gate[0, :, cut], nt, preferred_element_type=F32)
        up_pre += lax.dot_general(scaled, w_up[0, :, cut], nt, preferred_element_type=F32)
    scale = lax.rsqrt(square / (m * width) + epsilon)
    gate_pre *= scale
    up_pre *= scale
    inner = gate_pre.shape[1]
    hidden[tp] = (gate_pre / (1.0 + jnp.exp(-gate_pre)) * up_pre).astype(BF16)
    shared = []
    for j, there in enumerate(others[:-1]):
        shared.append(
            send(hidden.at[tp], hidden.at[tp], hid_send.at[j], hid_recv.at[j], {"tp": there})
        )
    for copy in shared:
        copy.wait_recv()
    outputs = jnp.zeros((n * capacity, width), F32)
    for t in range(m):
        outputs += jnp.dot(
            hidden[t], w_down[0, t * inner : (t + 1) * inner, :], preferred_element_type=F32
        )
    ready[...] = outputs.reshape(n, capacity, width).astype(BF16)
    backs = []
    for d in range(1, n):
        peer = lax.rem(me + d, n)
        backs.append(
            send(
                ready.at[lax.rem(peer, 2) * rows + peer // 2],
                returned.at[me],
                back_send.at[d],
                back_recv.at[d],
                {"ep": peer},
            )
        )
    returned[me] = ready[core * rows + row]
    for copy in backs:
        copy.wait_recv()
    rows = returned[...].astype(F32).reshape(n * capacity, width)
    mixture = jnp.dot(
        combine, rows, preferred_element_type=F32, precision=lax.Precision.HIGHEST
    )
    out_ref[...] = (mixed.astype(F32) + mixture).astype(BF16)
    for copy in parts + moved + joins + swaps + shared + backs:
        copy.wait_send()


def fused(
    stream,
    previous_state,
    mixer_norm_gain,
    query_matrix,
    key_matrix,
    value_matrix,
    output_gate_weight,
    decay_lower_factor,
    decay_upper_factor,
    forgetting_boost,
    head_norm_gain,
    output_matrix,
    mixture_norm_gain,
    expert_gate_weight,
    expert_up_weight,
    expert_down_weight,
    expert_index_table,
    expert_scores_within,
    group_probability,
):
    n = lax.axis_size("ep")
    m = lax.axis_size("tp")
    seqs, model = stream.shape
    width = previous_state.shape[2]
    span = width // DV * KEY_CHANNELS
    feats = query_matrix.shape[0]
    rank = decay_lower_factor.shape[1]
    steps = seqs // STEP
    total = 2 * span + 2 * width
    rows = n // 2
    half = rows * seqs
    dma = pltpu.SemaphoreType.DMA
    vmem = pl.BlockSpec(memory_space=pltpu.VMEM)
    hbm = pl.BlockSpec(memory_space=pltpu.HBM)
    fkq, values, gates = pl.pallas_call(
        functools.partial(project_kernel, n),
        name="project",
        out_shape=(
            jax.ShapeDtypeStruct((steps, 4 * STEP, span), F32),
            jax.ShapeDtypeStruct((steps, STEP, width), F32),
            jax.ShapeDtypeStruct((steps, STEP, width), F32),
        ),
        in_specs=[hbm] * 9,
        out_specs=(vmem,) * 3,
        scratch_shapes=[
            pltpu.VMEM((seqs, model), BF16),
            pltpu.VMEM((1, model), F32),
            pltpu.VMEM((feats, total), BF16),
            pltpu.VMEM((rank, model), BF16),
            pltpu.VMEM((rank, span), BF16),
            pltpu.VMEM((seqs, span), F32),
            pltpu.VMEM((n, seqs, feats), BF16),
            pltpu.VMEM((n, seqs, feats), BF16),
            pltpu.VMEM((half, total), BF16),
            pltpu.VMEM((half, total), BF16),
            pltpu.VMEM((rows, seqs, total), F32),
            pltpu.VMEM((rows, seqs, total), BF16),
            pltpu.VMEM((rows, seqs, total), BF16),
            dma((9,)),
            dma((n,)),
            dma((n,)),
            dma((3,)),
            dma((3,)),
            dma((3, rows)),
            dma((3, rows)),
        ],
        compiler_params=pltpu.CompilerParams(
            collective_id=0, has_side_effects=True, vmem_limit_bytes=12 * 2**20
        ),
        cost_estimate=pl.CostEstimate(flops=COST, bytes_accessed=3 * feats * total, transcendentals=0),
    )(
        *(pltpu.with_memory_space_constraint(a, pltpu.HBM) for a in (
            stream,
            mixer_norm_gain.reshape(1, model),
            query_matrix,
            key_matrix,
            value_matrix,
            output_gate_weight,
            decay_lower_factor.T,
            decay_upper_factor,
            forgetting_boost,
        ))
    )
    new_state, readout = pl.pallas_call(
        state_kernel,
        name="state",
        out_shape=(
            jax.ShapeDtypeStruct(previous_state.shape, F32),
            jax.ShapeDtypeStruct((seqs, 8, width), F32),
        ),
        in_specs=[vmem, vmem, vmem],
        out_specs=(hbm, vmem),
        scratch_shapes=[
            pltpu.VMEM((width // DV, KEY_CHANNELS, 4 * STEP), F32),
            pltpu.VMEM((2, STEP, KEY_CHANNELS, width), F32),
            dma((2,)),
        ],
        compiler_params=pltpu.CompilerParams(vmem_limit_bytes=6 * 2**20),
        cost_estimate=pl.CostEstimate(
            flops=COST // 4, bytes_accessed=4 * previous_state.size, transcendentals=0
        ),
    )(previous_state, fkq, values)
    inner = expert_gate_weight.shape[1]
    capacity = 2 * seqs * expert_index_table.shape[1] // n
    new_stream = pl.pallas_call(
        functools.partial(mixture_kernel, n, m),
        name="mixture",
        out_shape=jax.ShapeDtypeStruct((seqs, width), BF16),
        in_specs=[vmem] * 3 + [hbm] + [vmem] * 4 + [hbm] * 4,
        out_specs=vmem,
        scratch_shapes=[
            pltpu.VMEM((seqs, width), BF16),
            pltpu.VMEM((m, width, width), BF16),
            pltpu.VMEM(expert_gate_weight.shape, BF16),
            pltpu.VMEM(expert_up_weight.shape, BF16),
            pltpu.VMEM(expert_down_weight.shape, BF16),
            pltpu.VMEM((seqs, width), F32),
            pltpu.VMEM((m - 1, seqs, width), BF16),
            pltpu.VMEM((m - 1, seqs, width), BF16),
            pltpu.VMEM((GROUPS, capacity, width), BF16),
            pltpu.VMEM((m, 2, rows, capacity, width), BF16),
            pltpu.VMEM((m, n * capacity, inner), BF16),
            pltpu.VMEM((n, capacity, width), BF16),
            pltpu.VMEM((n, capacity, width), BF16),
            dma((m + 4,)),
            dma((m - 1,)),
            dma((m - 1,)),
            dma((rows,)),
            dma((rows,)),
            dma((m - 1,)),
            dma((m - 1,)),
            dma((m,)),
            dma((m,)),
            dma((m - 1,)),
            dma((m - 1,)),
            dma((n,)),
            dma((n,)),
        ],
        compiler_params=pltpu.CompilerParams(
            collective_id=1, has_side_effects=True, vmem_limit_bytes=VM3 * 2**20
        ),
        cost_estimate=pl.CostEstimate(flops=COST, bytes_accessed=2 * output_matrix.size, transcendentals=0),
    )(
        readout,
        gates,
        head_norm_gain.reshape(1, DV),
        stream,
        mixture_norm_gain.reshape(1, model),
        expert_index_table,
        expert_scores_within,
        group_probability.reshape(seqs, 1),
        *(
            pltpu.with_memory_space_constraint(a, pltpu.HBM)
            for a in (output_matrix, expert_gate_weight, expert_up_weight, expert_down_weight)
        ),
    )
    return (new_stream, new_state)


def on_device(*arrays):
    stream, state = arrays[0], arrays[1]
    experts_held, route_count = arrays[13].shape[0], arrays[16].shape[1]
    n = lax.axis_size("ep")
    whole_heads = state.shape[2] % DV == 0
    pair_routed = experts_held == 1 and n == GROUPS * route_count and route_count == 2
    full_tiles = stream.shape[0] % 16 == 0 and stream.shape[1] == state.shape[2] * lax.axis_size("tp")
    if whole_heads and pair_routed and full_tiles:
        return fused(*arrays)
    return general(*arrays)


def solution(mesh):
    placed = (
        P("ep", None),
        P("ep", None, "tp"),
        P(),
        P("ep", None),
        P("ep", None),
        P("ep", "tp"),
        P("ep", "tp"),
        P(),
        P(),
        P("ep", None),
        P(),
        P("tp", None),
        P(),
        P("ep", "tp", None),
        P("ep", "tp", None),
        P("ep", None, "tp"),
        P("ep", None),
        P("ep", None),
        P("ep"),
    )
    return jax.shard_map(
        on_device,
        mesh=mesh,
        in_specs=placed,
        out_specs=(P("ep", "tp"), P("ep", None, "tp")),
        check_vma=False,
    )
```

```python
import functools

import jax
import jax.numpy as jnp
from jax import lax
from jax.experimental import pallas as pl
from jax.experimental.pallas import tpu as pltpu
from jax.sharding import PartitionSpec as P

HEAD_TOTAL = 16
KEY_CHANNELS = 128
DV = 256
GROUPS = 4
STEP = 4
COST = 20_000_000_000
VM3 = 24
F32 = jnp.float32
BF16 = jnp.bfloat16
MESH = pl.DeviceIdType.MESH

epsilon = 1e-06
forgetting_softness = 16.0


def rms_scaled(values, gain_vec):
    floats = values.astype(jnp.float32)
    scaled = floats * lax.rsqrt(jnp.mean(floats * floats, axis=-1, keepdims=True) + epsilon)
    return (scaled * gain_vec).astype(jnp.bfloat16)


def general(
    stream,
    previous_state,
    mixer_norm_gain,
    query_matrix,
    key_matrix,
    value_matrix,
    output_gate_weight,
    decay_lower_factor,
    decay_upper_factor,
    forgetting_boost,
    head_norm_gain,
    output_matrix,
    mixture_norm_gain,
    expert_gate_weight,
    expert_up_weight,
    expert_down_weight,
    expert_index_table,
    expert_scores_within,
    group_probability,
):
    seq_count, model_width = stream.shape
    value_local = previous_state.shape[2]
    head_count = max(1, value_local // DV)
    head_width = min(value_local, DV)
    tp_index = lax.axis_index("tp")
    leading_head = tp_index * value_local // DV
    value_start = tp_index * value_local % DV
    key_column_span = head_count * KEY_CHANNELS
    normed = rms_scaled(stream, mixer_norm_gain)
    own_query = lax.dynamic_slice_in_dim(
        query_matrix, leading_head * KEY_CHANNELS, key_column_span, 1
    )
    own_key = lax.dynamic_slice_in_dim(key_matrix, leading_head * KEY_CHANNELS, key_column_span, 1)
    spread = lax.all_to_all(normed, "ep", split_axis=1, concat_axis=0, tiled=True)
    joined = jnp.concatenate([own_query, own_key, value_matrix, output_gate_weight], axis=1)
    summed = lax.psum_scatter(
        jnp.dot(spread, joined, preferred_element_type=jnp.float32),
        "ep",
        scatter_dimension=0,
        tiled=True,
    )
    query_sum = summed[:, :key_column_span]
    key_sum = summed[:, key_column_span : 2 * key_column_span]
    value_sum = summed[:, 2 * key_column_span : 2 * key_column_span + value_local]
    gate_sum = summed[:, 2 * key_column_span + value_local :]
    queries = (query_sum * KEY_CHANNELS ** (-0.5)).astype(jnp.bfloat16)
    key_rows = key_sum.astype(jnp.bfloat16)
    value_rows = value_sum.astype(jnp.bfloat16)
    gate_rows = gate_sum.astype(jnp.bfloat16)
    low_rank = jnp.dot(normed, decay_lower_factor, preferred_element_type=jnp.float32).astype(
        jnp.bfloat16
    )
    local_expand_matrix = lax.dynamic_slice_in_dim(
        decay_upper_factor, leading_head * KEY_CHANNELS, key_column_span, 1
    )
    forgetting_logit = jnp.dot(low_rank, local_expand_matrix, preferred_element_type=jnp.float32)
    request_boost = lax.dynamic_slice_in_dim(
        forgetting_boost, leading_head * KEY_CHANNELS, key_column_span, 1
    )
    forgetting_lograte = jax.nn.log_sigmoid(forgetting_logit) / forgetting_softness - request_boost
    factor = (
        jnp.exp(forgetting_lograte)
        .reshape(seq_count, head_count, KEY_CHANNELS)
        .transpose(0, 2, 1)[..., None]
    )
    state_four = previous_state.reshape(seq_count, KEY_CHANNELS, head_count, head_width)
    key_part = (
        key_rows.astype(jnp.float32)
        .reshape(seq_count, head_count, KEY_CHANNELS)
        .transpose(0, 2, 1)[..., None]
    )
    value_part = value_rows.astype(jnp.float32).reshape(seq_count, 1, head_count, head_width)
    updated = factor * state_four + key_part * value_part
    query_part = (
        queries.astype(jnp.float32).reshape(seq_count, head_count, KEY_CHANNELS).transpose(0, 2, 1)
    )
    readout = jnp.einsum("skh,skhv->shv", query_part, updated, precision=lax.Precision.HIGHEST)
    square_sums = jnp.sum(readout * readout, axis=-1)
    norm_table = lax.dynamic_update_slice(
        jnp.zeros((seq_count, HEAD_TOTAL), jnp.float32), square_sums, (jnp.int32(0), leading_head)
    )
    totals = lax.psum(norm_table, "tp")
    own_totals = lax.dynamic_slice_in_dim(totals, leading_head, head_count, 1)
    mean_sq = own_totals[..., None] / DV
    own_gain = lax.dynamic_slice_in_dim(head_norm_gain, value_start, head_width, 0)
    gate_part = jax.nn.silu(
        gate_rows.astype(jnp.float32).reshape(seq_count, head_count, head_width)
    )
    gated_rows = (
        (readout * lax.rsqrt(mean_sq + epsilon) * own_gain * gate_part)
        .reshape(seq_count, value_local)
        .astype(jnp.bfloat16)
    )
    partial_out = jnp.dot(gated_rows, output_matrix, preferred_element_type=jnp.float32)
    mixer_sum = lax.psum(partial_out.astype(jnp.bfloat16), "tp").astype(jnp.float32)
    blended_tokens = (stream.astype(jnp.float32) + mixer_sum).astype(jnp.bfloat16)
    normed_two = rms_scaled(blended_tokens, mixture_norm_gain)
    ep_count = lax.axis_size("ep")
    local_experts = expert_gate_weight.shape[0]
    experts_all = ep_count * local_experts
    route_count = expert_index_table.shape[1]
    capacity = 2 * seq_count * route_count // experts_all
    slot_count = experts_all * capacity
    flat_ids = expert_index_table.reshape(seq_count * route_count)
    one_hot = (flat_ids[:, None] == jnp.arange(experts_all, dtype=jnp.int32)[None, :]).astype(
        jnp.int32
    )
    rank_in = jnp.sum(one_hot * (jnp.cumsum(one_hot, axis=0) - 1), axis=1)
    place_lookup = flat_ids * capacity + rank_in
    placing = (place_lookup[:, None] == jnp.arange(slot_count, dtype=jnp.int32)[None, :]).astype(
        jnp.float32
    )
    placing = placing.reshape(seq_count, route_count, slot_count)
    logit_exp = jnp.exp(expert_scores_within)
    weights = logit_exp / jnp.sum(logit_exp, axis=-1, keepdims=True) * group_probability[:, None]
    combine = jnp.einsum("sk,skc->sc", weights, placing, precision=lax.Precision.HIGHEST)
    dispatch = jnp.sum(placing, axis=1).astype(jnp.bfloat16)
    outgoing = jnp.einsum("sc,sd->cd", dispatch, normed_two, preferred_element_type=jnp.float32)
    outgoing = outgoing.astype(jnp.bfloat16).reshape(experts_all, capacity, model_width)
    width_local = expert_down_weight.shape[2]
    arrived = lax.all_to_all(outgoing, "ep", split_axis=0, concat_axis=0, tiled=True)
    held_slots = arrived.shape[1]
    grouped = arrived.reshape(ep_count, local_experts, held_slots, model_width)
    gate_pre = jnp.einsum(
        "sxcd,xfd->sxcf", grouped, expert_gate_weight, preferred_element_type=jnp.float32
    )
    up_pre = jnp.einsum(
        "sxcd,xfd->sxcf", grouped, expert_up_weight, preferred_element_type=jnp.float32
    )
    hidden = (jax.nn.silu(gate_pre) * up_pre).astype(jnp.bfloat16)
    outputs = jnp.einsum(
        "sxcf,xfd->sxcd",
        lax.all_gather(hidden, "tp", axis=3, tiled=True),
        expert_down_weight,
        preferred_element_type=jnp.float32,
    )
    ready_rows = outputs.astype(jnp.bfloat16).reshape(
        ep_count * local_experts, held_slots, width_local
    )
    returned = lax.all_to_all(ready_rows, "ep", split_axis=0, concat_axis=0, tiled=True)
    mixture = jnp.dot(
        combine,
        returned.reshape(slot_count, width_local).astype(jnp.float32),
        precision=lax.Precision.HIGHEST,
    )
    own_mixed = lax.dynamic_slice_in_dim(blended_tokens, tp_index * width_local, width_local, 1)
    new_stream = (own_mixed.astype(jnp.float32) + mixture).astype(jnp.bfloat16)
    return (new_stream, updated.reshape(seq_count, KEY_CHANNELS, value_local))


def greet(partners):
    barrier = pltpu.get_barrier_semaphore()
    for partner in partners:
        pl.semaphore_signal(barrier, inc=1, device_id=partner, device_id_type=MESH)
    pl.semaphore_wait(barrier, len(partners))


def send(source, target, send_sem, recv_sem, partner):
    copy = pltpu.make_async_remote_copy(
        src_ref=source,
        dst_ref=target,
        send_sem=send_sem,
        recv_sem=recv_sem,
        device_id=partner,
        device_id_type=MESH,
    )
    copy.start()
    return copy


def project_kernel(
    n,
    stream_hbm,
    gain_hbm,
    query_hbm,
    key_hbm,
    value_hbm,
    gate_hbm,
    lower_hbm,
    upper_hbm,
    boost_hbm,
    fkq_ref,
    value_ref,
    gate_ref,
    stream,
    gain,
    weights,
    lower,
    upper,
    boost,
    chunks,
    spread,
    pair_out,
    pair_in,
    own,
    plane_out,
    plane_in,
    load_sem,
    chunk_send,
    chunk_recv,
    pair_send,
    pair_recv,
    plane_send,
    plane_recv,
):
    me = lax.axis_index("ep")
    tp = lax.axis_index("tp")
    core = lax.rem(me, 2)
    row = me // 2
    rows = n // 2
    seqs = stream.shape[0]
    feats = chunks.shape[2]
    span = boost.shape[1]
    width = value_hbm.shape[1]
    columns = pl.ds(pl.multiple_of(tp * span, 128), span)
    loads = [
        pltpu.make_async_copy(query_hbm.at[:, columns], weights.at[:, pl.ds(0, span)], load_sem.at[0]),
        pltpu.make_async_copy(key_hbm.at[:, columns], weights.at[:, pl.ds(span, span)], load_sem.at[1]),
        pltpu.make_async_copy(value_hbm, weights.at[:, pl.ds(2 * span, width)], load_sem.at[2]),
        pltpu.make_async_copy(gate_hbm, weights.at[:, pl.ds(2 * span + width, width)], load_sem.at[3]),
        pltpu.make_async_copy(lower_hbm, lower, load_sem.at[4]),
        pltpu.make_async_copy(upper_hbm.at[:, columns], upper, load_sem.at[5]),
        pltpu.make_async_copy(boost_hbm.at[:, columns], boost, load_sem.at[6]),
    ]
    first = [
        pltpu.make_async_copy(stream_hbm, stream, load_sem.at[7]),
        pltpu.make_async_copy(gain_hbm, gain, load_sem.at[8]),
    ]
    for load in first + loads:
        load.start()
    greet([{"ep": lax.rem(me + d, n)} for d in range(1, n)])
    for load in first:
        load.wait()
    floats = stream[...].astype(F32)
    scale = lax.rsqrt(jnp.mean(floats * floats, axis=-1, keepdims=True) + epsilon)
    normed = (floats * scale * gain[...]).astype(BF16)
    for d in range(n):
        chunks[d] = normed[:, d * feats : (d + 1) * feats]
    sent = []
    for d in range(1, n):
        peer = lax.rem(me + d, n)
        slot = row + rows * (d % 2)
        sent.append(
            send(chunks.at[peer], spread.at[slot], chunk_send.at[d], chunk_recv.at[d], {"ep": peer})
        )
    spread[row] = chunks[me]
    for load in loads[4:]:
        load.wait()
    nt = (((1,), (1,)), ((), ()))
    low_rank = lax.dot_general(normed, lower[...], nt, preferred_element_type=F32).astype(BF16)
    logit = jnp.dot(low_rank, upper[...], preferred_element_type=F32)
    log_sig = jnp.minimum(logit, 0.0) - jnp.log1p(jnp.exp(-jnp.abs(logit)))
    factor = jnp.exp(log_sig / forgetting_softness - boost[...])
    for load in loads[:4]:
        load.wait()
    for copy in sent:
        copy.wait_recv()
    half = rows * seqs
    x = spread[...].reshape(n * seqs, feats)
    cuts = [(0, 2 * span), (2 * span, width), (2 * span + width, width)]
    partner = {"ep": me + 1 - 2 * core}
    pairs = []
    for b, (start, size) in enumerate(cuts):
        part = jnp.dot(x, weights[:, start : start + size], preferred_element_type=F32)
        pair_out[:, start : start + size] = part[half:].astype(BF16)
        own[:, :, start : start + size] = part[:half].reshape(rows, seqs, size)
        at = (slice(None), pl.ds(start, size))
        pairs.append(
            send(pair_out.at[at], pair_in.at[at], pair_send.at[b], pair_recv.at[b], partner)
        )
    planes = []
    for b, (start, size) in enumerate(cuts):
        pairs[b].wait_recv()
        both = own[:, :, start : start + size] + pair_in[:, start : start + size].astype(
            F32
        ).reshape(rows, seqs, size)
        own[:, :, start : start + size] = both
        plane_out[:, :, start : start + size] = both.astype(BF16)
        for d in range(1, rows):
            there = lax.rem(row + d, rows)
            planes.append(
                send(
                    plane_out.at[there, :, pl.ds(start, size)],
                    plane_in.at[d, :, pl.ds(start, size)],
                    plane_send.at[b, d],
                    plane_recv.at[b, d],
                    {"ep": there * 2 + core},
                )
            )
    steps = seqs // STEP
    for b, (start, size) in enumerate(cuts):
        total = own[row, :, start : start + size]
        for d in range(1, rows):
            planes[b * (rows - 1) + d - 1].wait_recv()
            total = total + plane_in[d, :, start : start + size].astype(F32)
        if b == 0:
            query = (total[:, :span] * KEY_CHANNELS ** (-0.5)).astype(BF16).astype(F32)
            key = total[:, span:].astype(BF16).astype(F32)
            for i in range(steps):
                cut = slice(i * STEP, (i + 1) * STEP)
                fkq_ref[i, 0:STEP] = factor[cut]
                fkq_ref[i, STEP : 2 * STEP] = key[cut]
                fkq_ref[i, 2 * STEP : 3 * STEP] = query[cut]
                fkq_ref[i, 3 * STEP : 4 * STEP] = query[cut]
        else:
            target = value_ref if b == 1 else gate_ref
            total = total.astype(BF16).astype(F32)
            for i in range(steps):
                target[i] = total[i * STEP : (i + 1) * STEP]
    for copy in sent + pairs + planes:
        copy.wait_send()


def state_kernel(state_ref, fkq_ref, value_ref, new_hbm, read_ref, turned, buffer, out_sem):
    seqs, _, width = state_ref.shape
    heads = width // DV
    steps = seqs // STEP

    def flush(i, slot):
        return pltpu.make_async_copy(
            buffer.at[slot], new_hbm.at[pl.ds(i * STEP, STEP)], out_sem.at[slot]
        )

    @pl.loop(0, steps)
    def _(i):
        slot = lax.rem(i, 2)

        @pl.when(i >= 2)
        def _():
            flush(i - 2, slot).wait()

        for h in range(heads):
            turned[h] = fkq_ref[i, :, h * KEY_CHANNELS : (h + 1) * KEY_CHANNELS].T
        for s in range(STEP):
            sums = []
            for h in range(heads):
                lanes = slice(h * DV, (h + 1) * DV)
                factor = turned[h, :, s : s + 1]
                key = turned[h, :, STEP + s : STEP + s + 1]
                query = turned[h, :, 2 * STEP + s : 2 * STEP + s + 1]
                updated = factor * state_ref[i * STEP + s, :, lanes] + key * value_ref[
                    i, s : s + 1, lanes
                ]
                buffer[slot, s, :, lanes] = updated
                sums.append(jnp.sum((query * updated).reshape(-1, 8, DV), axis=0))
            read_ref[i * STEP + s] = jnp.concatenate(sums, axis=1)
        flush(i, slot).start()

    for i in range(steps - 2, steps):
        flush(i, i % 2).wait()


def mixture_kernel(
    n,
    m,
    read_ref,
    rows_ref,
    head_gain_ref,
    stream_hbm,
    gain_ref,
    index_ref,
    score_ref,
    prob_ref,
    output_hbm,
    gate_hbm,
    up_hbm,
    down_hbm,
    out_ref,
    own_stream,
    w_out,
    w_gate,
    w_up,
    w_down,
    lhs,
    part_out,
    part_in,
    slots_out,
    arrived,
    hidden,
    ready,
    returned,
    load_sem,
    part_send,
    part_recv,
    slot_send,
    slot_recv,
    join_send,
    join_recv,
    swap_send,
    swap_recv,
    hid_send,
    hid_recv,
    back_send,
    back_recv,
):
    me = lax.axis_index("ep")
    tp = lax.axis_index("tp")
    seqs, width = own_stream.shape
    rows = n // 2
    capacity = slots_out.shape[1]
    others = [lax.rem(tp + d, m) for d in range(1, m)] + [tp]
    own_cut = pl.ds(pl.multiple_of(tp * width, 128), width)
    load = pltpu.make_async_copy(stream_hbm.at[:, own_cut], own_stream, load_sem.at[m + 3])
    loads = []
    for j, there in enumerate(others):
        cut = pl.ds(pl.multiple_of(there * width, 128), width)
        loads.append(pltpu.make_async_copy(output_hbm.at[:, cut], w_out.at[j], load_sem.at[j]))
    loads += [
        pltpu.make_async_copy(gate_hbm, w_gate, load_sem.at[m]),
        pltpu.make_async_copy(up_hbm, w_up, load_sem.at[m + 1]),
        pltpu.make_async_copy(down_hbm, w_down, load_sem.at[m + 2]),
    ]
    for one in loads + [load]:
        one.start()
    for i in range(seqs // STEP):
        lhs[i * STEP : (i + 1) * STEP] = rows_ref[i]
    gates = lhs[...]
    silu = gates / (1.0 + jnp.exp(-gates))
    readout = jnp.sum(read_ref[...], axis=1)
    for h in range(width // DV):
        lanes = slice(h * DV, (h + 1) * DV)
        part = readout[:, lanes]
        mean_sq = jnp.mean(part * part, axis=-1, keepdims=True)
        lhs[:, lanes] = part * lax.rsqrt(mean_sq + epsilon) * head_gain_ref[...] * silu[:, lanes]
    gated = lhs[...].astype(BF16)
    greet(
        [{"tp": there} for there in others[:-1]]
        + [{"ep": lax.rem(me + d, n)} for d in range(1, n)]
    )
    parts = []
    for j, there in enumerate(others):
        loads[j].wait()
        part = jnp.dot(gated, w_out[j], preferred_element_type=F32)
        if j < m - 1:
            part_out[j] = part.astype(BF16)
            parts.append(
                send(part_out.at[j], part_in.at[j], part_send.at[j], part_recv.at[j], {"tp": there})
            )

    index = index_ref[...]
    group = index[:, 0:1] // (n // GROUPS)
    lane = lax.broadcasted_iota(jnp.int32, (seqs, 128), 1)
    one_hot = (lane == group).astype(F32)
    earlier = lax.broadcasted_iota(jnp.int32, (seqs, seqs), 1) < lax.broadcasted_iota(
        jnp.int32, (seqs, seqs), 0
    )
    counts = jnp.dot(earlier.astype(F32), one_hot, preferred_element_type=F32)
    rank = jnp.sum(counts * one_hot, axis=1, keepdims=True).astype(jnp.int32)
    slot_lane = lax.broadcasted_iota(jnp.int32, (seqs, GROUPS * capacity), 1)
    placing = (slot_lane == group * capacity + rank).astype(F32)
    scores = jnp.exp(score_ref[...])
    weights = scores / jnp.sum(scores, axis=-1, keepdims=True) * prob_ref[...]
    back_lane = lax.broadcasted_iota(jnp.int32, (seqs, n * capacity), 1)
    combine = jnp.zeros((seqs, n * capacity), F32)
    for k in range(index.shape[1]):
        combine += jnp.where(
            back_lane == index[:, k : k + 1] * capacity + rank, weights[:, k : k + 1], 0.0
        )

    load.wait()
    total = part
    for j in range(m - 1):
        parts[j].wait_recv()
        total = total + part_in[j].astype(F32)
    mixed = (own_stream[...].astype(F32) + total).astype(BF16)
    slots = lax.dot_general(
        placing, mixed.astype(F32), (((0,), (0,)), ((), ())), preferred_element_type=F32
    )
    slots_out[...] = slots.reshape(GROUPS, capacity, width).astype(BF16)
    core = lax.rem(me, 2)
    row = me // 2
    moved = []
    for d in range(1, rows):
        there = lax.rem(row + d, rows)
        moved.append(
            send(
                slots_out.at[there],
                arrived.at[tp, core, row],
                slot_send.at[d],
                slot_recv.at[d],
                {"ep": there * 2 + core},
            )
        )
    arrived[tp, core, row] = slots_out[row]
    for copy in moved:
        copy.wait_recv()
    joins = []
    for j, there in enumerate(others[:-1]):
        joins.append(
            send(
                arrived.at[tp, core],
                arrived.at[tp, core],
                join_send.at[j],
                join_recv.at[j],
                {"tp": there},
            )
        )
    for one in loads[m:]:
        one.wait()
    swaps = []
    nt = (((1,), (1,)), ((), ()))
    tokens_held = n * capacity
    square = jnp.zeros((tokens_held, 1), F32)
    gate_pre = jnp.zeros((tokens_held, w_gate.shape[1]), F32)
    up_pre = jnp.zeros((tokens_held, w_gate.shape[1]), F32)
    origin = [tp] + [lax.rem(tp - 1 - j + m, m) for j in range(m - 1)]
    for j, t in enumerate(origin):
        if j > 0:
            joins[j - 1].wait_recv()
        swaps.append(
            send(
                arrived.at[t, core],
                arrived.at[t, core],
                swap_send.at[j],
                swap_recv.at[j],
                {"ep": me + 1 - 2 * core},
            )
        )
    for j, t in enumerate(origin):
        swaps[j].wait_recv()
        cut = pl.ds(pl.multiple_of(t * width, 128), width)
        tokens = arrived[t].astype(F32).reshape(tokens_held, width)
        square += jnp.sum(tokens * tokens, axis=-1, keepdims=True)
        scaled = (tokens * gain_ref[:, cut]).astype(BF16)
        gate_pre += lax.dot_general(scaled, w_gate[0, :, cut], nt, preferred_element_type=F32)
        up_pre += lax.dot_general(scaled, w_up[0, :, cut], nt, preferred_element_type=F32)
    scale = lax.rsqrt(square / (m * width) + epsilon)
    gate_pre *= scale
    up_pre *= scale
    inner = gate_pre.shape[1]
    hidden[tp] = (gate_pre / (1.0 + jnp.exp(-gate_pre)) * up_pre).astype(BF16)
    shared = []
    for j, there in enumerate(others[:-1]):
        shared.append(
            send(hidden.at[tp], hidden.at[tp], hid_send.at[j], hid_recv.at[j], {"tp": there})
        )
    for copy in shared:
        copy.wait_recv()
    outputs = jnp.zeros((n * capacity, width), F32)
    for t in range(m):
        outputs += jnp.dot(
            hidden[t], w_down[0, t * inner : (t + 1) * inner, :], preferred_element_type=F32
        )
    ready[...] = outputs.reshape(n, capacity, width).astype(BF16)
    backs = []
    for d in range(1, n):
        peer = lax.rem(me + d, n)
        backs.append(
            send(
                ready.at[lax.rem(peer, 2) * rows + peer // 2],
                returned.at[me],
                back_send.at[d],
                back_recv.at[d],
                {"ep": peer},
            )
        )
    returned[me] = ready[core * rows + row]
    for copy in backs:
        copy.wait_recv()
    rows = returned[...].astype(F32).reshape(n * capacity, width)
    mixture = jnp.dot(
        combine, rows, preferred_element_type=F32, precision=lax.Precision.HIGHEST
    )
    out_ref[...] = (mixed.astype(F32) + mixture).astype(BF16)
    for copy in parts + moved + joins + swaps + shared + backs:
        copy.wait_send()


def fused(
    stream,
    previous_state,
    mixer_norm_gain,
    query_matrix,
    key_matrix,
    value_matrix,
    output_gate_weight,
    decay_lower_factor,
    decay_upper_factor,
    forgetting_boost,
    head_norm_gain,
    output_matrix,
    mixture_norm_gain,
    expert_gate_weight,
    expert_up_weight,
    expert_down_weight,
    expert_index_table,
    expert_scores_within,
    group_probability,
):
    n = lax.axis_size("ep")
    m = lax.axis_size("tp")
    seqs, model = stream.shape
    width = previous_state.shape[2]
    span = width // DV * KEY_CHANNELS
    feats = query_matrix.shape[0]
    rank = decay_lower_factor.shape[1]
    steps = seqs // STEP
    total = 2 * span + 2 * width
    rows = n // 2
    half = rows * seqs
    dma = pltpu.SemaphoreType.DMA
    vmem = pl.BlockSpec(memory_space=pltpu.VMEM)
    hbm = pl.BlockSpec(memory_space=pltpu.HBM)
    fkq, values, gates = pl.pallas_call(
        functools.partial(project_kernel, n),
        name="project",
        out_shape=(
            jax.ShapeDtypeStruct((steps, 4 * STEP, span), F32),
            jax.ShapeDtypeStruct((steps, STEP, width), F32),
            jax.ShapeDtypeStruct((steps, STEP, width), F32),
        ),
        in_specs=[hbm] * 9,
        out_specs=(vmem,) * 3,
        scratch_shapes=[
            pltpu.VMEM((seqs, model), BF16),
            pltpu.VMEM((1, model), F32),
            pltpu.VMEM((feats, total), BF16),
            pltpu.VMEM((rank, model), BF16),
            pltpu.VMEM((rank, span), BF16),
            pltpu.VMEM((seqs, span), F32),
            pltpu.VMEM((n, seqs, feats), BF16),
            pltpu.VMEM((n, seqs, feats), BF16),
            pltpu.VMEM((half, total), BF16),
            pltpu.VMEM((half, total), BF16),
            pltpu.VMEM((rows, seqs, total), F32),
            pltpu.VMEM((rows, seqs, total), BF16),
            pltpu.VMEM((rows, seqs, total), BF16),
            dma((9,)),
            dma((n,)),
            dma((n,)),
            dma((3,)),
            dma((3,)),
            dma((3, rows)),
            dma((3, rows)),
        ],
        compiler_params=pltpu.CompilerParams(
            collective_id=0, has_side_effects=True, vmem_limit_bytes=12 * 2**20
        ),
        cost_estimate=pl.CostEstimate(flops=COST, bytes_accessed=3 * feats * total, transcendentals=0),
    )(
        *(pltpu.with_memory_space_constraint(a, pltpu.HBM) for a in (
            stream,
            mixer_norm_gain.reshape(1, model),
            query_matrix,
            key_matrix,
            value_matrix,
            output_gate_weight,
            decay_lower_factor.T,
            decay_upper_factor,
            forgetting_boost,
        ))
    )
    new_state, readout = pl.pallas_call(
        state_kernel,
        name="state",
        out_shape=(
            jax.ShapeDtypeStruct(previous_state.shape, F32),
            jax.ShapeDtypeStruct((seqs, 8, width), F32),
        ),
        in_specs=[vmem, vmem, vmem],
        out_specs=(hbm, vmem),
        scratch_shapes=[
            pltpu.VMEM((width // DV, KEY_CHANNELS, 4 * STEP), F32),
            pltpu.VMEM((2, STEP, KEY_CHANNELS, width), F32),
            dma((2,)),
        ],
        compiler_params=pltpu.CompilerParams(vmem_limit_bytes=10 * 2**20),
        cost_estimate=pl.CostEstimate(
            flops=COST // 4, bytes_accessed=4 * previous_state.size, transcendentals=0
        ),
    )(previous_state, fkq, values)
    inner = expert_gate_weight.shape[1]
    capacity = 2 * seqs * expert_index_table.shape[1] // n
    new_stream = pl.pallas_call(
        functools.partial(mixture_kernel, n, m),
        name="mixture",
        out_shape=jax.ShapeDtypeStruct((seqs, width), BF16),
        in_specs=[vmem] * 3 + [hbm] + [vmem] * 4 + [hbm] * 4,
        out_specs=vmem,
        scratch_shapes=[
            pltpu.VMEM((seqs, width), BF16),
            pltpu.VMEM((m, width, width), BF16),
            pltpu.VMEM(expert_gate_weight.shape, BF16),
            pltpu.VMEM(expert_up_weight.shape, BF16),
            pltpu.VMEM(expert_down_weight.shape, BF16),
            pltpu.VMEM((seqs, width), F32),
            pltpu.VMEM((m - 1, seqs, width), BF16),
            pltpu.VMEM((m - 1, seqs, width), BF16),
            pltpu.VMEM((GROUPS, capacity, width), BF16),
            pltpu.VMEM((m, 2, rows, capacity, width), BF16),
            pltpu.VMEM((m, n * capacity, inner), BF16),
            pltpu.VMEM((n, capacity, width), BF16),
            pltpu.VMEM((n, capacity, width), BF16),
            dma((m + 4,)),
            dma((m - 1,)),
            dma((m - 1,)),
            dma((rows,)),
            dma((rows,)),
            dma((m - 1,)),
            dma((m - 1,)),
            dma((m,)),
            dma((m,)),
            dma((m - 1,)),
            dma((m - 1,)),
            dma((n,)),
            dma((n,)),
        ],
        compiler_params=pltpu.CompilerParams(
            collective_id=1, has_side_effects=True, vmem_limit_bytes=VM3 * 2**20
        ),
        cost_estimate=pl.CostEstimate(flops=COST, bytes_accessed=2 * output_matrix.size, transcendentals=0),
    )(
        readout,
        gates,
        head_norm_gain.reshape(1, DV),
        stream,
        mixture_norm_gain.reshape(1, model),
        expert_index_table,
        expert_scores_within,
        group_probability.reshape(seqs, 1),
        *(
            pltpu.with_memory_space_constraint(a, pltpu.HBM)
            for a in (output_matrix, expert_gate_weight, expert_up_weight, expert_down_weight)
        ),
    )
    return (new_stream, new_state)


def on_device(*arrays):
    stream, state = arrays[0], arrays[1]
    experts_held, route_count = arrays[13].shape[0], arrays[16].shape[1]
    n = lax.axis_size("ep")
    whole_heads = state.shape[2] % DV == 0
    pair_routed = experts_held == 1 and n == GROUPS * route_count and route_count == 2
    full_tiles = stream.shape[0] % 16 == 0 and stream.shape[1] == state.shape[2] * lax.axis_size("tp")
    if whole_heads and pair_routed and full_tiles:
        return fused(*arrays)
    return general(*arrays)


def solution(mesh):
    placed = (
        P("ep", None),
        P("ep", None, "tp"),
        P(),
        P("ep", None),
        P("ep", None),
        P("ep", "tp"),
        P("ep", "tp"),
        P(),
        P(),
        P("ep", None),
        P(),
        P("tp", None),
        P(),
        P("ep", "tp", None),
        P("ep", "tp", None),
        P("ep", None, "tp"),
        P("ep", None),
        P("ep", None),
        P("ep"),
    )
    return jax.shard_map(
        on_device,
        mesh=mesh,
        in_specs=placed,
        out_specs=(P("ep", "tp"), P("ep", None, "tp")),
        check_vma=False,
    )
```
